32 devices in a mesh: sp: 16 (over z, y, x), tp: 2 (over core).
Axes of the slice: x: 2, y: 2, z: 4, core: 2. Of those that a mesh axis runs over, the one named last changes fastest.
Arguments:
- tokens: bfloat16 [4096, 2048], P(('sp', 'tp')), may hold values from -6 to 6
- norm_gain: float32 [2048], replicated, may hold values from 0.1 to 1.9
- w_query: bfloat16 [2048, 2048], P('sp', 'tp'), may hold values from -0.125 to 0.125
- w_key: bfloat16 [2048, 2048], P('sp', 'tp'), may hold values from -0.125 to 0.125
- w_value: bfloat16 [2048, 4096], P('sp', 'tp'), may hold values from -0.125 to 0.125
- w_rank_down: bfloat16 [2048, 16], replicated, may hold values from -0.125 to 0.125
- w_rank_up: bfloat16 [16, 2048], P(None, 'tp'), may hold values from -1.5 to 1.5
- gate_bias: float32 [2048], P('tp')
- decay_shift: float32 [4096], P('sp'), may hold values from -1 to 0
- out_gain: float32 [512], replicated, may hold values from 0.1 to 1.9
- w_out: bfloat16 [4096, 2048], P('tp', 'sp'), may hold values from -0.09375 to 0.09375
Outputs:
- mixed: bfloat16 [4096, 2048], P(('sp', 'tp'))
The draws below stay inside these ranges and needn't reach their ends.
All inputs are finite; a program needn't handle non-finite values.
Results may differ from the reference program's by a relative error of at most 0.015.
Values may be sent and summed in bfloat16 or wider, within the bound.
A program may use at most 128 MiB of HBM per device.

```python
import jax
import jax.numpy as jnp
from jax import lax

D = 2048
HEADS = 8
DK = 256
DV = 512
RANK = 16
TAU = 16
BLOCK = 64
STRETCH = 256
TOKENS = 4096
KEYS = 2048
VALS = 4096
N_SP = 16
N_TP = 2


def draw_gate_bias(key, part):
    first, second, third = jax.random.split(key, 3)
    share = 0.5
    slow_head = jax.random.uniform(first, (HEADS,)) < share
    slow = jnp.log(2.0 * TOKENS / TAU) + jax.random.uniform(second, (HEADS, DK), minval=-0.5, maxval=0.5)
    fast = jax.random.uniform(third, (HEADS, DK), minval=0.5, maxval=1.5)
    return jnp.where(slow_head[:, None], slow, fast).reshape(HEADS * DK).astype(jnp.float32)


def draw_decay_shift(key, part):
    first, second, third, fourth = jax.random.split(key, 4)
    stretches = TOKENS // STRETCH
    level = jnp.exp(jax.random.uniform(first, (stretches,), minval=jnp.log(0.1), maxval=0.0))
    spread = jax.random.uniform(second, (TOKENS,), minval=0.5, maxval=1.5)
    per_position = -jnp.repeat(level, STRETCH) * spread / TOKENS
    spots = jax.random.randint(third, (3,), 0, TOKENS)
    drops = jnp.log(jax.random.uniform(fourth, (3,), minval=0.5, maxval=0.8))
    return per_position.at[spots].add(drops).astype(jnp.float32)


def shard_levels(stream_key, dims, cuts, least, top_value):
    def one(axis_at, parts):
        steps = jax.random.uniform(jax.random.fold_in(jax.random.fold_in(stream_key, 6), axis_at), (parts,), jnp.float32, least / len(cuts), top_value / len(cuts))
        return jnp.repeat(jnp.exp(steps), dims[axis_at] // parts).reshape((-1,) + (1,) * (len(dims) - axis_at - 1))

    factor_of = one(*cuts[0])
    for cut in cuts[1:]:
        factor_of = factor_of * one(*cut)
    return factor_of


def noise(own_key, extent, deviation, most, cuts=(), kind=jnp.bfloat16):
    array = deviation * jax.random.normal(own_key, extent, jnp.float32)
    if cuts:
        array = array * shard_levels(own_key, extent, cuts, -0.22, 0.18)
    return jnp.clip(array, -most, most).astype(kind)


def setup_inputs(seed: int = 0) -> dict:
    splits = jax.random.split(jax.random.key(seed), 12)
    tokens = noise(splits[0], (TOKENS, D), 1.0, 6.0, ((0, 32),))
    norm_gain = jnp.clip(1.0 + 0.18 * jax.random.normal(splits[1], (D,), jnp.float32), 0.1, 1.9)
    w_query = noise(splits[2], (D, KEYS), D ** -0.5, 0.125, ((0, 16), (1, 2)))
    w_key = noise(splits[3], (D, KEYS), D ** -0.5, 0.125, ((0, 16), (1, 2)))
    w_value = noise(splits[4], (D, VALS), D ** -0.5, 0.125, ((0, 16), (1, 2)))
    w_rank_down = noise(splits[5], (D, RANK), D ** -0.5, 0.125)
    w_rank_up = noise(splits[6], (RANK, KEYS), RANK ** -0.5, 1.5, ((1, 2),))
    gate_bias = draw_gate_bias(jax.random.fold_in(splits[11], 71), 0)
    decay_shift = draw_decay_shift(jax.random.fold_in(splits[11], 71), 0)
    out_gain = jnp.clip(1.0 + 0.18 * jax.random.normal(splits[9], (DV,), jnp.float32), 0.1, 1.9)
    w_out = noise(splits[10], (VALS, D), VALS ** -0.5, 0.09375, ((0, 2), (1, 16)))
    return dict(tokens=tokens, norm_gain=norm_gain, w_query=w_query, w_key=w_key, w_value=w_value, w_rank_down=w_rank_down, w_rank_up=w_rank_up, gate_bias=gate_bias, decay_shift=decay_shift, out_gain=out_gain, w_out=w_out)


EPS = 1e-06

def rms_rows(values, gain):
    wide = values.astype(jnp.float32)
    return wide * lax.rsqrt(lax.optimization_barrier(jnp.mean(wide * wide, axis=-1, keepdims=True)) + EPS) * gain

def narrow(values):
    return lax.optimization_barrier(values.astype(jnp.bfloat16)).astype(jnp.float32)

def local_pass(query, key, value, log_decay, state):
    rows, heads, width = query.shape
    blocks = rows // BLOCK

    def split(tensor):
        return tensor.reshape((blocks, BLOCK) + tensor.shape[1:])
    causal = jnp.tril(jnp.ones((BLOCK, BLOCK), dtype=bool))

    def step(carry, inputs):
        q_blk, k_blk, v_blk, g_blk = inputs
        cumul = jnp.cumsum(g_blk, axis=0)
        centre = cumul - cumul[BLOCK // 2]
        q_scaled = narrow(q_blk * jnp.exp(centre))
        k_scaled = narrow(k_blk * jnp.exp(-centre))
        scores = jnp.einsum('ihd,jhd->hij', q_scaled, k_scaled)
        scores = narrow(jnp.where(causal[None], scores, 0.0))
        within = jnp.einsum('hij,jhe->ihe', scores, v_blk)
        final = cumul[-1]
        decayed = narrow(k_blk * jnp.exp(final - cumul))
        nxt = jnp.exp(final)[:, :, None] * carry + jnp.einsum('jhd,jhe->hde', decayed, v_blk)
        return (nxt, (within, q_blk * jnp.exp(cumul), final, carry))
    carry, (within, reach, finals, starts) = lax.scan(step, state, (split(query), split(key), split(value), split(log_decay)))
    return (within, reach, finals, starts, carry)

def read_out(reach, starts):
    blocks, block, heads, width = reach.shape
    result = jnp.einsum('nihd,nhde->nihe', narrow(reach), narrow(starts))
    return result.reshape(blocks * block, heads, -1)

def reference(tokens, norm_gain, w_query, w_key, w_value, w_rank_down, w_rank_up, gate_bias, decay_shift, out_gain, w_out):
    group_width = HEADS // N_TP * DV

    def segment(state, inputs):
        rows, shift = inputs
        normed = rms_rows(rows, norm_gain).astype(jnp.bfloat16)
        query = jnp.dot(normed, w_query, preferred_element_type=jnp.float32).astype(jnp.bfloat16)
        keyed = jnp.dot(normed, w_key, preferred_element_type=jnp.float32).astype(jnp.bfloat16)
        valued = jnp.dot(normed, w_value, preferred_element_type=jnp.float32).astype(jnp.bfloat16)
        rank = jnp.dot(normed, w_rank_down, preferred_element_type=jnp.float32).astype(jnp.bfloat16)
        pre = jnp.dot(rank, w_rank_up, preferred_element_type=jnp.float32) + gate_bias
        log_decay = jax.nn.log_sigmoid(pre) / TAU + shift[:, None]
        q_heads = query.astype(jnp.float32).reshape(STRETCH, HEADS, DK) * DK ** (-0.5)
        k_heads = keyed.astype(jnp.float32).reshape(STRETCH, HEADS, DK)
        v_heads = valued.astype(jnp.float32).reshape(STRETCH, HEADS, DV)
        within, reach, _, starts, state = local_pass(q_heads, k_heads, v_heads, log_decay.reshape(STRETCH, HEADS, DK), state)
        attended = within.reshape(STRETCH, HEADS, DV) + read_out(reach, starts)
        shaped = rms_rows(attended, out_gain).astype(jnp.bfloat16).reshape(STRETCH, VALS)
        total = jnp.zeros((STRETCH, D), jnp.float32)
        for group in range(N_TP):
            lower = group * group_width
            part = jnp.dot(shaped[:, lower:lower + group_width], w_out[lower:lower + group_width], preferred_element_type=jnp.float32).astype(jnp.bfloat16)
            total = total + lax.optimization_barrier(part).astype(jnp.float32)
        return (state, total.astype(jnp.bfloat16))
    start = jnp.zeros((HEADS, DK, DV), jnp.float32)
    _, mixed = lax.scan(segment, start, (tokens.reshape(N_SP, STRETCH, D), decay_shift.reshape(N_SP, STRETCH)))
    return mixed.reshape(TOKENS, D)
```

```python
import functools

import jax
import jax.numpy as jnp
from jax import lax
from jax.experimental import pallas as pl
from jax.experimental.pallas import tpu as pltpu
from jax.sharding import PartitionSpec as P

DK = 256
DV = 512
KV = DK + DV
TAU = 16
BLOCK = 64
EPS = 1e-06
CHUNKS = 4
MESH = pl.DeviceIdType.MESH
VMEM = pl.BlockSpec(memory_space=pltpu.VMEM)
LIMIT = 60 * 2**20
NT = (((1,), (1,)), ((), ()))
TN = (((0,), (0,)), ((), ()))


class Plan:
    def __init__(self, n, tp, heads):
        self.n, self.tp, self.heads = n, tp, heads
        bits = [1 << k for k in range(n.bit_length() - 1)]
        order = [b for b in (1, 4, 2) if b in bits] + [b for b in bits if b > 4]
        self.team = sorted(order[: heads.bit_length() - 1])
        self.span = sorted((b for b in bits if b not in self.team), reverse=True)
        self.bits = bits
        self.run = 1
        while self.run in self.team:
            self.run *= 2
        self.blocks = heads // self.run
        self.spread = [0]
        for b in self.span:
            self.spread = self.spread + [s | b for s in self.spread]

    def mask(self, d):
        return sum(b for k, b in enumerate(self.team) if d >> k & 1)

    def hop(self, s):
        return max((k for k, b in enumerate(self.span) if s & b), default=-1)

    def flip(self, index, mask):
        for b in self.bits:
            if mask & b:
                index = index + b * (1 - 2 * ((index // b) % 2))
        return index

    def member(self, index):
        return sum((((index // b) % 2) << k for k, b in enumerate(self.team)), 0 * index)

    def other(self, member, d):
        for k in range(len(self.team)):
            b = 1 << k
            member = member + b * (1 - 2 * ((member // b) % 2)) * ((d // b) % 2)
        return member

    def base(self, index, t):
        for k, b in enumerate(self.team):
            index = index - b * ((index // b) % 2) + b * (t * self.run >> k & 1)
        return index


def greet(devices):
    barrier = pltpu.get_barrier_semaphore()
    for device in devices:
        pl.semaphore_signal(barrier, inc=1, device_id=device, device_id_type=MESH)
    pl.semaphore_wait(barrier, len(devices))


class Mail:
    def __init__(self, send_sem, recv_sem):
        self.send_sem, self.recv_sem, self.out = send_sem, recv_sem, []

    def send(self, src, dst, device, slot):
        copy = pltpu.make_async_remote_copy(
            src_ref=src,
            dst_ref=dst,
            send_sem=self.send_sem.at[len(self.out)],
            recv_sem=self.recv_sem.at[slot],
            device_id=device,
            device_id_type=MESH,
        )
        copy.start()
        self.out.append(copy)

    def receive(self, dst, device, slot):
        pltpu.make_async_remote_copy(
            src_ref=dst,
            dst_ref=dst,
            send_sem=self.send_sem.at[0],
            recv_sem=self.recv_sem.at[slot],
            device_id=device,
            device_id_type=MESH,
        ).wait_recv()

    def finish(self):
        for copy in self.out:
            copy.wait_send()


def layer_kernel(
    plan, staged, tokens, gain, shift, wq, wk, wv, wo, down, up, bias, out_gain, out,
    X, SH, W, WO, acc_kv, acc_q, G, Kb, Vb, carries, within, reach, ends, logs, hold, starts,
    sent, got, sent_log, got_log, shaped, part, from_core, total, sum_out, sum_in,
    kv_send, kv_recv, q_send, q_recv, o_send, o_recv, x_send, x_recv, s_send, s_recv, r_send, r_recv, local_sem,
):
    n, tp, heads, run, blocks = plan.n, plan.tp, plan.heads, plan.run, plan.blocks
    me, core = lax.axis_index("sp"), lax.axis_index("tp")
    rows, cols = wq.shape[0], wo.shape[1]
    share = tokens.shape[0]
    seg = share * tp
    cores = [lax.rem(core + e, tp) for e in range(1, tp)]
    back = [lax.rem(core + tp - e, tp) for e in range(1, tp)]
    peers = [plan.flip(me, plan.mask(d)) for d in range(heads)]
    mine = plan.member(me)
    last_hop = len(plan.span) - 1
    greet(
        [(p, core) for p in peers[1:]]
        + [(plan.flip(me, b), core) for b in plan.span]
        + [(me, c) for c in cores]
    )
    mail_kv, mail_q, mail_o, mail_x = Mail(kv_send, kv_recv), Mail(q_send, q_recv), Mail(o_send, o_recv), Mail(x_send, x_recv)
    base_s, base_c = heads, 2 * heads

    def lines(index):
        return pl.ds(pl.multiple_of(index * rows, rows), rows)

    def kv_at(index):
        return W.at[lines(index), 0:KV]

    def q_at(index):
        return W.at[lines(index), KV:]

    def o_at(index):
        if len(WO.shape) == 3:
            return WO.at[index]
        return WO.at[:, pl.ds(pl.multiple_of(index * cols, cols), cols)]

    def kv_from(j):
        place = lines(me)
        return [
            (wk.at[:, pl.ds(pl.multiple_of(j * DK, DK), DK)], W.at[place, 0:DK]),
            (wv.at[:, pl.ds(pl.multiple_of(j * DV, DV), DV)], W.at[place, DK:KV]),
        ]

    def q_from(j):
        return [(wq.at[:, pl.ds(pl.multiple_of(j * DK, DK), DK)], W.at[lines(me), KV:])]

    def o_from(j):
        return [(wo.at[pl.ds(pl.multiple_of(j * DV, DV), DV), :], o_at(me))]

    def to_team(box, pairs):
        for d in range(1, heads):
            for src, dst in pairs(plan.member(peers[d])):
                box.send(src, dst, (peers[d], core), plan.mask(d))

    def own_out(box, pairs):
        for b in plan.span[::-1]:
            for src, dst in pairs(mine):
                box.send(src, dst, (plan.flip(me, b), core), b)

    def await_piece(box, view, s, d):
        if s == 0 and d == 0:
            return
        mask = s | plan.mask(d)
        hop = plan.hop(s)
        sender = peers[d] if hop < 0 else plan.flip(me, plan.span[hop])
        box.receive(view(plan.flip(me, mask)), (sender, core), mask)

    def hand_over(box, view, s, d):
        mask = s | plan.mask(d)
        source = plan.flip(me, mask)
        for later in range(plan.hop(s) + 1, last_hop + 1):
            bit = plan.span[later]
            box.send(view(source), view(source), (plan.flip(me, bit), core), mask ^ bit)

    def forward(box, view, s, d):
        await_piece(box, view, s, d)
        hand_over(box, view, s, d)

    def slot_rows(member, c):
        return pl.ds(pl.multiple_of((member * tp + c) * share, share), share)

    def slot(index, c):
        return X.at[slot_rows(plan.member(index), c), :]

    locals_ = []
    for at, (src, dst) in enumerate(kv_from(mine) + q_from(mine) + o_from(mine)):
        copy = pltpu.make_async_copy(src, dst, local_sem.at[at])
        copy.start()
        locals_.append(copy)
    to_team(mail_kv, kv_from)
    own_out(mail_kv, kv_from)
    raw = tokens[...].astype(jnp.float32)
    raw = raw * lax.rsqrt(jnp.mean(raw * raw, axis=-1, keepdims=True) + EPS) * gain[...]
    X[slot_rows(mine, core), :] = raw.astype(jnp.bfloat16)
    SH[mine] = jnp.broadcast_to(shift[...], SH.shape[1:])

    def token_on(d, top):
        for k in range(top):
            mail_x.send(slot(peers[d], core), slot(peers[d], core), (peers[1 << k], core), d ^ (1 << k))
        for e, c in enumerate(cores):
            mail_x.send(slot(peers[d], core), slot(peers[d], core), (me, c), base_c + d * (tp - 1) + e)

    def token_in(d):
        k = d.bit_length() - 1
        low = (d & -d).bit_length() - 1
        mail_x.receive(slot(peers[d], core), (peers[1 << low], core), d)
        token_on(d, low)

    def token_ready(d):
        for e, c in enumerate(back):
            mail_x.receive(slot(peers[d], c), (me, c), base_c + d * (tp - 1) + e)
        if d:
            mail_x.receive(SH.at[plan.member(peers[d])], (peers[d], core), base_s + d)

    token_on(0, len(plan.team))
    for d in range(1, heads):
        mail_x.send(SH.at[mine], SH.at[mine], (peers[d], core), base_s + d)
    to_team(mail_q, q_from)
    for copy in locals_:
        copy.wait()

    tile = min(seg, 256)
    tiles = seg // tile
    row = lax.broadcasted_iota(jnp.int32, (tile, tile), 0)
    col = lax.broadcasted_iota(jnp.int32, (tile, tile), 1)
    lower = (row >= col) & (row // BLOCK == col // BLOCK)
    ones = jnp.where(lower, 1.0, 0.0).astype(jnp.bfloat16)
    causal = lax.broadcasted_iota(jnp.int32, (BLOCK, BLOCK), 0) >= lax.broadcasted_iota(jnp.int32, (BLOCK, BLOCK), 1)
    up_here = up[:, pl.ds(pl.multiple_of(mine * DK, DK), DK)]
    bias_here = bias[:, pl.ds(pl.multiple_of(mine * DK, DK), DK)]

    def gates(d, t):
        i = plan.other(mine, d)
        at = pl.ds(pl.multiple_of(i * seg + t * tile, tile), tile)
        rank = lax.dot_general(X[at, :], down[...], NT, preferred_element_type=jnp.float32)
        pre = jnp.dot(rank.astype(jnp.bfloat16), up_here, preferred_element_type=jnp.float32) + bias_here
        gate = (jnp.minimum(pre, 0.0) - jnp.log1p(jnp.exp(-jnp.abs(pre)))) / TAU
        moved = SH[i, 0:1, pl.ds(pl.multiple_of(t * tile, tile), tile)]
        first = gate.astype(jnp.bfloat16)
        rest = gate - first.astype(jnp.float32)
        second = rest.astype(jnp.bfloat16)
        third = (rest - second.astype(jnp.float32)).astype(jnp.bfloat16)
        G[at, :] = (
            jnp.dot(ones, first, preferred_element_type=jnp.float32)
            + jnp.dot(ones, second, preferred_element_type=jnp.float32)
            + jnp.dot(ones, third, preferred_element_type=jnp.float32)
            + jnp.sum(jnp.where(lower, moved, 0.0), axis=1, keepdims=True)
        )

    def gates_of(low, high):
        def body(step, nothing):
            gates(low + step // tiles, step % tiles)
            return nothing

        lax.fori_loop(0, (high - low) * tiles, body, 0)

    def term(at, s, lo, hi):
        if staged:
            value = None
            for t in range(heads // run):
                place = plan.base(plan.flip(me, s), t) * rows
                span = pl.ds(pl.multiple_of(place, rows * run), rows * run)
                one = jnp.dot(X[at, span], W[span, lo:hi], preferred_element_type=jnp.float32)
                value = one if value is None else value + one
            return value
        return jnp.dot(X[at, :], W[:, lo:hi], preferred_element_type=jnp.float32)

    def accumulate(acc, lo, hi, s, first, low, high):
        def body(step, nothing):
            i = plan.other(mine, low + step // tiles)
            at = pl.ds(pl.multiple_of(i * seg + (step % tiles) * tile, tile), tile)
            value = term(at, s, lo, hi)
            acc[at, :] = value if first else acc[at, :] + value
            return nothing

        lax.fori_loop(0, (high - low) * tiles, body, 0)

    spread = plan.spread
    early = [s for s in spread if not s or plan.hop(s) < last_hop]
    late = [s for s in spread if s not in early]
    for d in range(1, heads):
        forward(mail_kv, kv_at, 0, d)
    token_ready(0)
    gates_of(0, 1)
    order = [1 << k for k in range(len(plan.team))] + [d for d in range(heads) if d & (d - 1)]
    waiting = [(s, d) for s in early if s for d in range(heads)]
    half = len(waiting) // 2
    for s, d in waiting[:half]:
        forward(mail_kv, kv_at, s, d)
    for d in order:
        if d & (d - 1) == 0:
            token_in(d)
    for s, d in waiting[half:]:
        forward(mail_kv, kv_at, s, d)
    own_out(mail_q, q_from)
    for d in range(1, heads):
        forward(mail_q, q_at, 0, d)
    to_team(mail_o, o_from)
    solo = [d for d in order if d & (d - 1) == 0]
    for d in solo:
        token_ready(d)
        gates_of(d, d + 1)
    near_heads = len(solo) + 1 if heads > 1 else 1
    near_heads = min(near_heads, 3) if heads > 2 else heads
    if staged:
        for at, s in enumerate(spread[:-1]):
            if s in late:
                for d in range(heads):
                    await_piece(mail_kv, kv_at, s, d)
            accumulate(acc_kv, 0, KV, s, at == 0, 0, near_heads)
    for d in order:
        if d & (d - 1):
            token_in(d)
            token_ready(d)
            gates_of(d, d + 1)
    if staged:
        for at, s in enumerate(spread[:-1]):
            accumulate(acc_kv, 0, KV, s, at == 0, near_heads, heads)
        for d in range(heads):
            await_piece(mail_kv, kv_at, spread[-1], d)
    else:
        for s in late:
            for d in range(heads):
                await_piece(mail_kv, kv_at, s, d)

    per_run = run * tiles
    ends[...] = jnp.zeros_like(ends)
    logs[...] = jnp.zeros_like(logs)

    def keys(index, nothing):
        u = index // per_run
        at = pl.ds(pl.multiple_of(index * tile, tile), tile)
        joined = term(at, spread[-1], 0, KV)
        if staged:
            joined = joined + acc_kv[at, :]
        joined = joined.astype(jnp.bfloat16)
        Kb[at, :] = joined[:, :DK]
        Vb[at, :] = joined[:, DK:]
        carry, past = ends[u], logs[u, 0:1, :]
        for b in range(tile // BLOCK):
            here = slice(b * BLOCK, (b + 1) * BLOCK)
            place = pl.ds(pl.multiple_of(index * tile + b * BLOCK, BLOCK), BLOCK)
            cumul = G[place, :]
            final = cumul[BLOCK - 1 : BLOCK]
            carries[index * (tile // BLOCK) + b] = carry.astype(jnp.bfloat16)
            decayed = (joined[here, :DK].astype(jnp.float32) * jnp.exp(final - cumul)).astype(jnp.bfloat16)
            carry = jnp.exp(final) * carry + lax.dot_general(
                joined[here, DK:], decayed, TN, preferred_element_type=jnp.float32
            )
            past = past + final
        ends[u] = carry
        logs[u] = jnp.broadcast_to(past, logs.shape[1:])
        return nothing

    lax.fori_loop(0, heads * tiles, keys, 0)

    mail_s = Mail(s_send, s_recv)
    depth = DV // CHUNKS

    def scan(c):
        piece = slice(c * depth, (c + 1) * depth)
        ahead = [jnp.zeros((1, DK), jnp.float32)] * blocks
        spans = [logs[u, 0:1, :] for u in range(blocks)]
        groups = [[u] for u in range(blocks)]
        for u in range(blocks):
            hold[u, piece, :] = jnp.zeros((depth, DK), jnp.float32)
        at = 0
        for bit in plan.bits:
            if bit < run:
                continue
            if bit in plan.team:
                merged, span = [], []
                for a in range(0, len(groups), 2):
                    one, two = groups[a], groups[a + 1]
                    value = ends[one[0], piece, :]
                    for i in two:
                        hold[i, piece, :] = hold[i, piece, :] + jnp.exp(ahead[i]) * value
                        ahead[i] = ahead[i] + spans[a]
                    ends[one[0], piece, :] = jnp.exp(spans[a + 1]) * value + ends[two[0], piece, :]
                    span.append(spans[a] + spans[a + 1])
                    merged.append(one + two)
                groups, spans = merged, span
                continue
            partner = (plan.flip(me, bit), core)
            high = (me // bit) % 2 == 1
            for u, g in enumerate(groups):
                if c == 0:
                    sent_log[at + u] = jnp.broadcast_to(spans[u], sent_log.shape[1:])
                    mail_s.send(sent_log.at[at + u], got_log.at[at + u], partner, (CHUNKS + 1) * (at + u))
                sent[at + u, piece, :] = ends[g[0], piece, :].astype(jnp.bfloat16)
                mail_s.send(
                    sent.at[at + u, piece, :], got.at[at + u, piece, :], partner, (CHUNKS + 1) * (at + u) + 1 + c
                )
            yield
            for u, g in enumerate(groups):
                if c == 0:
                    mail_s.receive(got_log.at[at + u], partner, (CHUNKS + 1) * (at + u))
                mail_s.receive(got.at[at + u, piece, :], partner, (CHUNKS + 1) * (at + u) + 1 + c)
                value = got[at + u, piece, :].astype(jnp.float32)
                value_log = got_log[at + u, 0:1, :]
                for i in g:
                    hold[i, piece, :] = hold[i, piece, :] + jnp.where(high, jnp.exp(ahead[i]), 0.0) * value
                    ahead[i] = ahead[i] + jnp.where(high, value_log, 0.0)
                if bit != plan.bits[-1]:
                    ends[g[0], piece, :] = (
                        jnp.exp(jnp.where(high, 0.0, value_log)) * ends[g[0], piece, :]
                        + jnp.exp(jnp.where(high, spans[u], 0.0)) * value
                    )
                    spans[u] = spans[u] + value_log
            at += len(groups)
        for u in range(blocks):
            starts[u, piece, :] = hold[u, piece, :].astype(jnp.bfloat16)
        yield

    scans = [scan(c) for c in range(CHUNKS)]
    steps = len([b for b in plan.bits if b not in plan.team])

    def step_scans():
        for one in scans:
            next(one)

    step_scans()
    for s in early:
        if s:
            for d in range(heads):
                forward(mail_q, q_at, s, d)
    first_o = [d for d in range(heads)]
    cut = (heads + 1) // 2
    own_out(mail_o, o_from)
    for d in first_o[1:cut]:
        forward(mail_o, o_at, 0, d)
    for s in late:
        for d in range(heads):
            await_piece(mail_q, q_at, s, d)

    def queries(index, nothing):
        u = index // per_run
        at = pl.ds(pl.multiple_of(index * tile, tile), tile)
        joined = term(at, spread[0], KV, KV + DK)
        if staged:
            for s in spread[1:]:
                joined = joined + term(at, s, KV, KV + DK)
        joined = joined.astype(jnp.bfloat16).astype(jnp.float32) * DK ** (-0.5)
        past = acc_q[0:1, :]
        past = jnp.where(index % per_run == 0, 0.0, past)
        for b in range(tile // BLOCK):
            here = slice(b * BLOCK, (b + 1) * BLOCK)
            place = pl.ds(pl.multiple_of(index * tile + b * BLOCK, BLOCK), BLOCK)
            q = joined[here]
            k = Kb[place, :].astype(jnp.float32)
            cumul = G[place, :]
            centre = cumul - cumul[BLOCK // 2 : BLOCK // 2 + 1]
            final = cumul[BLOCK - 1 : BLOCK]
            q_scaled = (q * jnp.exp(centre)).astype(jnp.bfloat16)
            k_scaled = (k * jnp.exp(-centre)).astype(jnp.bfloat16)
            scores = lax.dot_general(q_scaled, k_scaled, NT, preferred_element_type=jnp.float32)
            scores = jnp.where(causal, scores, 0.0).astype(jnp.bfloat16)
            near = (q * jnp.exp(cumul)).astype(jnp.bfloat16)
            within[place, :] = jnp.dot(scores, Vb[place, :], preferred_element_type=jnp.float32) + lax.dot_general(
                near, carries[index * (tile // BLOCK) + b], NT, preferred_element_type=jnp.float32
            )
            reach[place, :] = (q * jnp.exp(cumul + past)).astype(jnp.bfloat16)
            past = past + final
        acc_q[0:1, :] = past
        return nothing

    acc_q[...] = jnp.zeros_like(acc_q)
    middle = heads * tiles // 2
    lax.fori_loop(0, middle, queries, 0)
    if steps:
        step_scans()
    for d in first_o[max(cut, 1) :]:
        forward(mail_o, o_at, 0, d)
    lax.fori_loop(middle, heads * tiles, queries, 0)
    for s in early:
        if s:
            for d in range(cut):
                forward(mail_o, o_at, s, d)
    for _ in range(steps - 1):
        step_scans()

    def shape(index, nothing):
        u = index // per_run
        at = pl.ds(pl.multiple_of(index * tile, tile), tile)
        wide = within[at, :] + lax.dot_general(reach[at, :], starts[u], NT, preferred_element_type=jnp.float32)
        value = wide * lax.rsqrt(jnp.mean(wide * wide, axis=-1, keepdims=True) + EPS) * out_gain[...]
        value = value.astype(jnp.bfloat16)
        if tile == seg:
            for c in range(tp):
                to = pl.ds(pl.multiple_of((c * heads + index) * share, share), share)
                shaped[to, :] = value[c * share : (c + 1) * share]
        else:
            for p in range(tile // share):
                lot = index * (tile // share) + p
                to = pl.ds(pl.multiple_of(((lot % tp) * heads + lot // tp) * share, share), share)
                shaped[to, :] = value[p * share : (p + 1) * share]
        return nothing

    lax.fori_loop(0, heads * tiles, shape, 0)

    mail_r = Mail(r_send, r_recv)
    lots = heads * share
    width = out.shape[1]
    groups = [[s] for s in spread] if staged else [spread]
    fields = heads // run

    def product(c, group):
        left = shaped[pl.ds(pl.multiple_of(c * lots, lots), lots), :]
        if staged:
            right = []
            for t in range(fields):
                place = plan.base(plan.flip(me, group[0]), t) * cols
                right.append(WO[:, pl.ds(pl.multiple_of(place, run * cols), run * cols)])
            return [jnp.dot(left, one, preferred_element_type=jnp.float32) for one in right]
        if len(WO.shape) == 3:
            return [jnp.dot(left, WO[s], preferred_element_type=jnp.float32) for s in range(n)]
        return [jnp.dot(left, WO[...], preferred_element_type=jnp.float32)]

    def spots(values):
        at, result = 0, []
        for value in values:
            result.append(slice(at, at + value.shape[1]))
            at += value.shape[1]
        return result

    per_group = heads * tp + heads
    for g, group in enumerate(groups):
        for s in group:
            if s in late:
                for d in range(heads):
                    await_piece(mail_o, o_at, s, d)
            elif s:
                for d in range(cut, heads):
                    forward(mail_o, o_at, s, d)
        for e, c in enumerate(cores):
            values = product(c, group)
            for place, value in zip(spots(values), values):
                part[g, e, :, place] = value.astype(jnp.bfloat16)
            mail_r.send(part.at[g, e], from_core.at[g, e], (me, c), g * per_group + e)
        values = product(core, group)
        for place, value in zip(spots(values), values):
            total[g, :, place] = value
        for e, c in enumerate(back):
            mail_r.receive(from_core.at[g, e], (me, c), g * per_group + e)
            total[g] = total[g] + from_core[g, e].astype(jnp.float32)
        if heads > 1:
            sum_out[g] = total[g].astype(jnp.bfloat16)
        for d in range(heads - 1, 0, -1):
            lot = pl.ds(pl.multiple_of(plan.member(peers[d]) * share, share), share)
            mail_r.send(sum_out.at[g, lot, :], sum_in.at[g, d - 1], (peers[d], core), g * per_group + heads * tp + d)
    for g, group in enumerate(groups):
        lot = pl.ds(pl.multiple_of(mine * share, share), share)
        value = total[g, lot, :]
        for d in range(heads - 1, 0, -1):
            mail_r.receive(sum_in.at[g, d - 1], (peers[d], core), g * per_group + heads * tp + d)
            value = value + sum_in[g, d - 1].astype(jnp.float32)
        value = value.astype(jnp.bfloat16)
        if staged:
            for t in range(fields):
                place = plan.base(plan.flip(me, group[0]), t) * cols
                out[:, pl.ds(pl.multiple_of(place, run * cols), run * cols)] = value[:, t * run * cols : (t + 1) * run * cols]
        else:
            out[...] = value
    for box in (mail_kv, mail_q, mail_o, mail_x, mail_s, mail_r):
        box.finish()


def on_device(
    tokens, norm_gain, w_query, w_key, w_value, w_rank_down, w_rank_up, gate_bias, decay_shift, out_gain, w_out
):
    n, tp = lax.axis_size("sp"), lax.axis_size("tp")
    heads = w_query.shape[1] // DK
    plan = Plan(n, tp, heads)
    rows, width = tokens.shape
    deep = w_query.shape[0]
    seg = rows * tp
    count = heads * seg
    dma, vmem = pltpu.SemaphoreType.DMA, pltpu.VMEM
    cols = w_out.shape[1]
    aligned = cols % 128 == 0
    staged = aligned and len(plan.span) > 0 and plan.run * deep % 256 == 0
    groups = len(plan.spread) if staged else 1
    field = width // groups
    most = max(1, plan.blocks * len(plan.span))
    given = max(1, tp - 1)
    bf16, f32 = jnp.bfloat16, jnp.float32
    slots = 2 * n + 8 * (heads + len(plan.span))
    tokens_sent = heads * (tp + 2 + len(plan.team))
    return pl.pallas_call(
        functools.partial(layer_kernel, plan, staged),
        out_shape=jax.ShapeDtypeStruct((rows, width), bf16),
        in_specs=[VMEM] * 11,
        out_specs=VMEM,
        scratch_shapes=[
            vmem((count, width), bf16),
            vmem((heads, 8, seg), f32),
            vmem((n * deep, KV + DK), bf16),
            vmem((DV, n * cols) if aligned else (n, DV, cols), bf16),
            vmem((count, KV) if staged else (8, 128), f32),
            vmem((8, DK), f32),
            vmem((count, DK), f32),
            vmem((count, DK), bf16),
            vmem((count, DV), bf16),
            vmem((count // BLOCK, DV, DK), bf16),
            vmem((count, DV), f32),
            vmem((count, DK), bf16),
            vmem((plan.blocks, DV, DK), f32),
            vmem((plan.blocks, 8, DK), f32),
            vmem((plan.blocks, DV, DK), f32),
            vmem((plan.blocks, DV, DK), bf16),
            vmem((most, DV, DK), bf16),
            vmem((most, DV, DK), bf16),
            vmem((most, 8, DK), f32),
            vmem((most, 8, DK), f32),
            vmem((count, DV), bf16),
            vmem((groups, given, heads * rows, field), bf16),
            vmem((groups, given, heads * rows, field), bf16),
            vmem((groups, heads * rows, field), f32),
            vmem((groups, heads * rows, field) if heads > 1 else (1, 16, 128), bf16),
            vmem((groups, max(1, heads - 1), rows, field) if heads > 1 else (1, 1, 16, 128), bf16),
            dma((slots,)),
            dma((n,)),
            dma((slots,)),
            dma((n,)),
            dma((slots,)),
            dma((n,)),
            dma((tokens_sent,)),
            dma((heads * (tp + 2),)),
            dma(((CHUNKS + 1) * most,)),
            dma(((CHUNKS + 1) * most,)),
            dma((groups * (heads + tp),)),
            dma((groups * (heads * tp + heads),)),
            dma((4,)),
        ],
        compiler_params=pltpu.CompilerParams(
            collective_id=0, has_side_effects=True, vmem_limit_bytes=LIMIT
        ),
        name="layer",
    )(
        tokens,
        norm_gain[None],
        decay_shift[None],
        w_query,
        w_key,
        w_value,
        w_out,
        w_rank_down.T,
        w_rank_up,
        gate_bias[None],
        out_gain[None],
    )


def solution(mesh):
    return jax.shard_map(
        on_device,
        mesh=mesh,
        in_specs=(
            P(("sp", "tp"), None),
            P(),
            P("sp", "tp"),
            P("sp", "tp"),
            P("sp", "tp"),
            P(),
            P(None, "tp"),
            P("tp"),
            P("sp"),
            P(),
            P("tp", "sp"),
        ),
        out_specs=P(("sp", "tp"), None),
        check_vma=False,
    )
```

```python
import functools

import jax
import jax.numpy as jnp
from jax import lax
from jax.experimental import pallas as pl
from jax.experimental.pallas import tpu as pltpu
from jax.sharding import PartitionSpec as P

DK = 256
DV = 512
KV = DK + DV
TAU = 16
BLOCK = 64
EPS = 1e-06
CHUNKS = 4
MESH = pl.DeviceIdType.MESH
VMEM = pl.BlockSpec(memory_space=pltpu.VMEM)
LIMIT = 60 * 2**20
NT = (((1,), (1,)), ((), ()))
TN = (((0,), (0,)), ((), ()))


class Plan:
    def __init__(self, n, tp, heads):
        self.n, self.tp, self.heads = n, tp, heads
        bits = [1 << k for k in range(n.bit_length() - 1)]
        order = [b for b in (1, 4, 2) if b in bits] + [b for b in bits if b > 4]
        self.team = sorted(order[: heads.bit_length() - 1])
        self.span = sorted((b for b in bits if b not in self.team), reverse=True)
        self.bits = bits
        self.run = 1
        while self.run in self.team:
            self.run *= 2
        self.blocks = heads // self.run
        self.line = self.team == [1, 4] and self.span == [8, 2]
        self.spread = [0]
        for b in self.span:
            self.spread = self.spread + [s | b for s in self.spread]

    def mask(self, d):
        return sum(b for k, b in enumerate(self.team) if d >> k & 1)

    def hop(self, s):
        return max((k for k, b in enumerate(self.span) if s & b), default=-1)

    def flip(self, index, mask):
        for b in self.bits:
            if mask & b:
                index = index + b * (1 - 2 * ((index // b) % 2))
        return index

    def member(self, index):
        return sum((((index // b) % 2) << k for k, b in enumerate(self.team)), 0 * index)

    def other(self, member, d):
        for k in range(len(self.team)):
            b = 1 << k
            member = member + b * (1 - 2 * ((member // b) % 2)) * ((d // b) % 2)
        return member

    def base(self, index, t):
        for k, b in enumerate(self.team):
            index = index - b * ((index // b) % 2) + b * (t * self.run >> k & 1)
        return index


def greet(devices):
    barrier = pltpu.get_barrier_semaphore()
    for device in devices:
        pl.semaphore_signal(barrier, inc=1, device_id=device, device_id_type=MESH)
    pl.semaphore_wait(barrier, len(devices))


class Mail:
    def __init__(self, send_sem, recv_sem):
        self.send_sem, self.recv_sem, self.out = send_sem, recv_sem, []

    def send(self, src, dst, device, slot, held=False, when=None):
        copy = pltpu.make_async_remote_copy(
            src_ref=src,
            dst_ref=dst,
            send_sem=self.send_sem.at[len(self.out)],
            recv_sem=self.recv_sem.at[slot],
            device_id=device,
            device_id_type=MESH,
        )
        if not held:
            copy.start()
        self.out.append((copy, when))
        return copy

    def receive(self, dst, device, slot):
        pltpu.make_async_remote_copy(
            src_ref=dst,
            dst_ref=dst,
            send_sem=self.send_sem.at[0],
            recv_sem=self.recv_sem.at[slot],
            device_id=device,
            device_id_type=MESH,
        ).wait_recv()

    def finish(self):
        for copy, when in self.out:
            if when is None:
                copy.wait_send()
            else:
                pl.when(when)(copy.wait_send)


def layer_kernel(
    plan, staged, tokens, gain, shift, wq, wk, wv, wo, down, up, bias, out_gain, out,
    X, SH, W, WO, acc_kv, acc_q, G, Kb, Vb, carries, within, reach, ends, logs, hold, starts,
    sent, got, sent_log, got_log, shaped, part, from_core, total, sum_out, sum_in,
    kv_send, kv_recv, q_send, q_recv, o_send, o_recv, x_send, x_recv, s_send, s_recv, r_send, r_recv, local_sem,
):
    n, tp, heads, run, blocks = plan.n, plan.tp, plan.heads, plan.run, plan.blocks
    me, core = lax.axis_index("sp"), lax.axis_index("tp")
    rows, cols = wq.shape[0], wo.shape[1]
    share = tokens.shape[0]
    seg = share * tp
    cores = [lax.rem(core + e, tp) for e in range(1, tp)]
    back = [lax.rem(core + tp - e, tp) for e in range(1, tp)]
    peers = [plan.flip(me, plan.mask(d)) for d in range(heads)]
    mine = plan.member(me)
    last_hop = len(plan.span) - 1
    greet(
        [(p, core) for p in peers[1:]]
        + [(plan.flip(me, b), core) for b in plan.span]
        + ([(plan.flip(me, 12), core)] if plan.line else [])
        + [(me, c) for c in cores]
    )
    mail_kv, mail_q, mail_o, mail_x = Mail(kv_send, kv_recv), Mail(q_send, q_recv), Mail(o_send, o_recv), Mail(x_send, x_recv)
    base_s, base_c = heads, 2 * heads

    def lines(index):
        return pl.ds(pl.multiple_of(index * rows, rows), rows)

    def kv_at(index, j=0):
        return W.at[j, lines(index), 0:KV]

    def q_at(index, j=0):
        return W.at[j, lines(index), KV:]

    def o_at(index, j=0):
        if len(WO.shape) == 4:
            return WO.at[j, index]
        return WO.at[j, :, pl.ds(pl.multiple_of(index * cols, cols), cols)]

    def kv_from(m, j=0):
        place = lines(me)
        return [
            (wk.at[:, pl.ds(pl.multiple_of(m * DK, DK), DK)], W.at[j, place, 0:DK]),
            (wv.at[:, pl.ds(pl.multiple_of(m * DV, DV), DV)], W.at[j, place, DK:KV]),
        ]

    def q_from(m, j=0):
        return [(wq.at[:, pl.ds(pl.multiple_of(m * DK, DK), DK)], W.at[j, lines(me), KV:])]

    def o_from(m, j=0):
        return [(wo.at[pl.ds(pl.multiple_of(m * DV, DV), DV), :], o_at(me, j))]

    plane = me // 4
    y_peer = (plan.flip(me, 2), core)

    def tag(dz, q, kind):
        return ((dz + 3) * 2 + q) * 3 + kind

    def source(dz, q, y):
        return plan.flip(me, q + 2 * y) + 4 * dz

    def room(sign):
        return (3 - plane, plane) if sign > 0 else (plane, 3 - plane)

    def line_open(box, pairs):
        for j in (0, 1):
            for src, dst in pairs(plan.other(mine, 1 + 2 * j), j):
                box.send(src, dst, (peers[1], core), tag(0, 1, j))

    def line_own_y(box, pairs):
        for src, dst in pairs(mine, 0):
            box.send(src, dst, y_peer, tag(0, 0, 2))

    def line_own_z(box, pairs):
        for j in (1, 0):
            for sign in (1, -1):
                test = room(sign)[0] >= 2 - j
                copies = [
                    box.send(src, dst, (me + 4 * sign, core), tag(-sign, 0, 1 - j), True, test)
                    for src, dst in pairs(plan.other(mine, 2 * j), 1 - j)
                ]
                start_if(test, copies)

    def line_x_y(box, view):
        for j in (0, 1):
            index = source(0, 1, 0)
            box.receive(view(index, j), (peers[1], core), tag(0, 1, j))
            if j == 0:
                box.send(view(index), view(index), y_peer, tag(0, 1, 2))

    def line_x_z(box, view):
        index = source(0, 1, 0)
        for j in (0, 1):
            for sign in (1, -1):
                test = room(sign)[0] >= 2 - j
                start_if(test, [
                    box.send(view(index, j), view(index, 1 - j), (me + 4 * sign, core), tag(-sign, 1, 1 - j), True, test)
                ])

    def line_step(box, view, k, q):
        for sign in (1, -1):
            ahead, behind = room(sign)
            for j in (0, 1):
                if k + j > 3:
                    continue
                index = source(-sign * k, q, 0)
                test = (behind >= k) & (ahead >= j)
                onward = (behind >= k) & (ahead >= 2 - j)
                over = [box.send(view(index), view(index), y_peer, tag(-sign * k, q, 2), True, test)] if j == 0 else []
                on = []
                if k + 2 - j <= 3:
                    on.append(
                        box.send(
                            view(index, j), view(index, 1 - j), (me + 4 * sign, core),
                            tag(-sign * (k + 1), q, 1 - j), True, onward,
                        )
                    )

                @pl.when(test)
                def _():
                    box.receive(view(index, j), (me - 4 * sign, core), tag(-sign * k, q, j))
                    for copy in over:
                        copy.start()

                if on:
                    start_if(onward, on)

    def line_await(box, view, gaps):
        for dz in gaps:
            for q in (0, 1):
                test = (plane + dz >= 0) & (plane + dz <= 3)

                @pl.when(test)
                def _():
                    box.receive(view(source(dz, q, 1)), y_peer, tag(dz, q, 2))

    def to_team(box, pairs):
        for d in range(1, heads):
            for src, dst in pairs(plan.member(peers[d])):
                box.send(src, dst, (peers[d], core), plan.mask(d))

    def own_out(box, pairs, bits, held=False):
        return [
            box.send(src, dst, (plan.flip(me, b), core), b, held) for b in bits for src, dst in pairs(mine)
        ]

    def start_if(test, copies):
        @pl.when(test)
        def _():
            for copy in copies:
                copy.start()

    def await_piece(box, view, s, d):
        if s == 0 and d == 0:
            return
        mask = s | plan.mask(d)
        hop = plan.hop(s)
        sender = peers[d] if hop < 0 else plan.flip(me, plan.span[hop])
        box.receive(view(plan.flip(me, mask)), (sender, core), mask)

    def hand_over(box, view, s, d):
        mask = s | plan.mask(d)
        source = plan.flip(me, mask)
        for later in range(plan.hop(s) + 1, last_hop + 1):
            bit = plan.span[later]
            box.send(view(source), view(source), (plan.flip(me, bit), core), mask ^ bit)

    def forward(box, view, s, d):
        await_piece(box, view, s, d)
        hand_over(box, view, s, d)

    def slot_rows(member, c):
        return pl.ds(pl.multiple_of((member * tp + c) * share, share), share)

    def slot(index, c):
        return X.at[slot_rows(plan.member(index), c), :]

    locals_ = []
    for at, (src, dst) in enumerate(kv_from(mine) + q_from(mine) + o_from(mine)):
        copy = pltpu.make_async_copy(src, dst, local_sem.at[at])
        copy.start()
        locals_.append(copy)
    line = plan.line
    if line:
        line_open(mail_kv, kv_from)
        line_own_y(mail_kv, kv_from)
        line_own_z(mail_kv, kv_from)
        line_open(mail_q, q_from)
        line_own_y(mail_q, q_from)
    else:
        to_team(mail_kv, kv_from)
        own_out(mail_kv, kv_from, plan.span)
        to_team(mail_q, q_from)
        own_out(mail_q, q_from, plan.span)
    raw = tokens[...].astype(jnp.float32)
    raw = raw * lax.rsqrt(jnp.mean(raw * raw, axis=-1, keepdims=True) + EPS) * gain[...]
    X[slot_rows(mine, core), :] = raw.astype(jnp.bfloat16)
    SH[mine] = jnp.broadcast_to(shift[...], SH.shape[1:])

    def token_on(d, top):
        for k in range(top):
            mail_x.send(slot(peers[d], core), slot(peers[d], core), (peers[1 << k], core), d ^ (1 << k))
        for e, c in enumerate(cores):
            mail_x.send(slot(peers[d], core), slot(peers[d], core), (me, c), base_c + d * (tp - 1) + e)

    def token_in(d):
        k = d.bit_length() - 1
        low = (d & -d).bit_length() - 1
        mail_x.receive(slot(peers[d], core), (peers[1 << low], core), d)
        token_on(d, low)

    def token_ready(d):
        for e, c in enumerate(back):
            mail_x.receive(slot(peers[d], c), (me, c), base_c + d * (tp - 1) + e)
        if d:
            mail_x.receive(SH.at[plan.member(peers[d])], (peers[d], core), base_s + d)

    token_on(0, len(plan.team))
    for d in range(1, heads):
        mail_x.send(SH.at[mine], SH.at[mine], (peers[d], core), base_s + d)
    for copy in locals_:
        copy.wait()

    tile = min(seg, 256)
    tiles = seg // tile
    row = lax.broadcasted_iota(jnp.int32, (tile, tile), 0)
    col = lax.broadcasted_iota(jnp.int32, (tile, tile), 1)
    lower = (row >= col) & (row // BLOCK == col // BLOCK)
    ones = jnp.where(lower, 1.0, 0.0).astype(jnp.bfloat16)
    causal = lax.broadcasted_iota(jnp.int32, (BLOCK, BLOCK), 0) >= lax.broadcasted_iota(jnp.int32, (BLOCK, BLOCK), 1)
    up_here = up[:, pl.ds(pl.multiple_of(mine * DK, DK), DK)]
    bias_here = bias[:, pl.ds(pl.multiple_of(mine * DK, DK), DK)]

    def gates(d, t):
        i = plan.other(mine, d)
        at = pl.ds(pl.multiple_of(i * seg + t * tile, tile), tile)
        rank = lax.dot_general(X[at, :], down[...], NT, preferred_element_type=jnp.float32)
        pre = jnp.dot(rank.astype(jnp.bfloat16), up_here, preferred_element_type=jnp.float32) + bias_here
        gate = (jnp.minimum(pre, 0.0) - jnp.log1p(jnp.exp(-jnp.abs(pre)))) / TAU
        moved = SH[i, 0:1, pl.ds(pl.multiple_of(t * tile, tile), tile)]
        first = gate.astype(jnp.bfloat16)
        rest = gate - first.astype(jnp.float32)
        second = rest.astype(jnp.bfloat16)
        third = (rest - second.astype(jnp.float32)).astype(jnp.bfloat16)
        G[at, :] = (
            jnp.dot(ones, first, preferred_element_type=jnp.float32)
            + jnp.dot(ones, second, preferred_element_type=jnp.float32)
            + jnp.dot(ones, third, preferred_element_type=jnp.float32)
            + jnp.sum(jnp.where(lower, moved, 0.0), axis=1, keepdims=True)
        )

    def gates_of(low, high):
        def body(step, nothing):
            gates(low + step // tiles, step % tiles)
            return nothing

        lax.fori_loop(0, (high - low) * tiles, body, 0)

    def term(at, s, lo, hi):
        if staged:
            value = None
            for t in range(heads // run):
                place = plan.base(plan.flip(me, s), t) * rows
                span = pl.ds(pl.multiple_of(place, rows * run), rows * run)
                one = jnp.dot(X[at, span], W[0, span, lo:hi], preferred_element_type=jnp.float32)
                value = one if value is None else value + one
            return value
        return jnp.dot(X[at, :], W[0, :, lo:hi], preferred_element_type=jnp.float32)

    def accumulate(acc, lo, hi, s, first, low, high):
        def body(step, nothing):
            i = plan.other(mine, low + step // tiles)
            at = pl.ds(pl.multiple_of(i * seg + (step % tiles) * tile, tile), tile)
            value = term(at, s, lo, hi)
            acc[at, :] = value if first else acc[at, :] + value
            return nothing

        lax.fori_loop(0, (high - low) * tiles, body, 0)

    spread = plan.spread
    early = [s for s in spread if not s or plan.hop(s) < last_hop]
    late = [s for s in spread if s not in early]
    solo = [1 << k for k in range(len(plan.team))]
    rest = [d for d in range(1, heads) if d not in solo]
    waiting = [(s, d) for s in early if s for d in range(heads)]
    if line:
        line_x_y(mail_kv, kv_at)
        line_x_z(mail_kv, kv_at)
        line_step(mail_kv, kv_at, 1, 0)
        token_ready(0)
        gates_of(0, 1)
        line_x_y(mail_q, q_at)
        line_own_y(mail_o, o_from)
        for d in solo:
            token_in(d)
        line_step(mail_kv, kv_at, 1, 1)
        line_open(mail_o, o_from)
        token_ready(1)
        gates_of(1, 2)
        line_step(mail_kv, kv_at, 2, 0)
        token_ready(2)
        gates_of(2, 3)
        line_step(mail_kv, kv_at, 2, 1)
        line_own_z(mail_q, q_from)
        line_x_z(mail_q, q_at)
        line_step(mail_kv, kv_at, 3, 0)
        line_step(mail_kv, kv_at, 3, 1)
    else:
        for d in range(1, heads):
            forward(mail_kv, kv_at, 0, d)
        token_ready(0)
        gates_of(0, 1)
        for d in range(1, heads):
            forward(mail_q, q_at, 0, d)
        to_team(mail_o, o_from)
        for d in solo:
            token_in(d)
        for d in solo:
            token_ready(d)
            gates_of(d, d + 1)
        for s, e in waiting:
            forward(mail_kv, kv_at, s, e)
    near_heads = 3 if heads > 2 else heads
    for d in rest:
        token_in(d)
    if staged:
        for at, s in enumerate(spread[:-1]):
            if s in late:
                if line:
                    line_await(mail_kv, kv_at, (0, 1, -1))
                else:
                    for d in range(heads):
                        await_piece(mail_kv, kv_at, s, d)
            accumulate(acc_kv, 0, KV, s, at == 0, 0, near_heads)
    for d in rest:
        token_ready(d)
        gates_of(d, d + 1)
    if line:
        for k in (1, 2, 3):
            for q in (0, 1):
                line_step(mail_q, q_at, k, q)
            if k == 2:
                line_own_z(mail_o, o_from)
                line_x_y(mail_o, o_at)
                line_x_z(mail_o, o_at)
    else:
        for s, e in waiting:
            forward(mail_q, q_at, s, e)
    if staged:
        for at, s in enumerate(spread[:-1]):
            accumulate(acc_kv, 0, KV, s, at == 0, near_heads, heads)
        if line:
            line_await(mail_kv, kv_at, (2, -2, 3, -3))
        else:
            for d in range(heads):
                await_piece(mail_kv, kv_at, spread[-1], d)
    else:
        for s in late:
            for d in range(heads):
                await_piece(mail_kv, kv_at, s, d)

    per_run = run * tiles
    ends[...] = jnp.zeros_like(ends)
    logs[...] = jnp.zeros_like(logs)

    def keys(index, nothing):
        u = index // per_run
        at = pl.ds(pl.multiple_of(index * tile, tile), tile)
        joined = term(at, spread[-1], 0, KV)
        if staged:
            joined = joined + acc_kv[at, :]
        joined = joined.astype(jnp.bfloat16)
        Kb[at, :] = joined[:, :DK]
        Vb[at, :] = joined[:, DK:]
        carry, past = ends[u], logs[u, 0:1, :]
        for b in range(tile // BLOCK):
            here = slice(b * BLOCK, (b + 1) * BLOCK)
            place = pl.ds(pl.multiple_of(index * tile + b * BLOCK, BLOCK), BLOCK)
            cumul = G[place, :]
            final = cumul[BLOCK - 1 : BLOCK]
            carries[index * (tile // BLOCK) + b] = carry.astype(jnp.bfloat16)
            decayed = (joined[here, :DK].astype(jnp.float32) * jnp.exp(final - cumul)).astype(jnp.bfloat16)
            carry = jnp.exp(final) * carry + lax.dot_general(
                joined[here, DK:], decayed, TN, preferred_element_type=jnp.float32
            )
            past = past + final
        ends[u] = carry
        logs[u] = jnp.broadcast_to(past, logs.shape[1:])
        return nothing

    lax.fori_loop(0, heads * tiles, keys, 0)

    mail_s = Mail(s_send, s_recv)
    depth = DV // CHUNKS

    def scan(c):
        piece = slice(c * depth, (c + 1) * depth)
        ahead = [jnp.zeros((1, DK), jnp.float32)] * blocks
        spans = [logs[u, 0:1, :] for u in range(blocks)]
        groups = [[u] for u in range(blocks)]
        for u in range(blocks):
            hold[u, piece, :] = jnp.zeros((depth, DK), jnp.float32)
        at = 0
        for bit in plan.bits:
            if bit < run:
                continue
            if bit in plan.team:
                merged, span = [], []
                for a in range(0, len(groups), 2):
                    one, two = groups[a], groups[a + 1]
                    value = ends[one[0], piece, :]
                    for i in two:
                        hold[i, piece, :] = hold[i, piece, :] + jnp.exp(ahead[i]) * value
                        ahead[i] = ahead[i] + spans[a]
                    ends[one[0], piece, :] = jnp.exp(spans[a + 1]) * value + ends[two[0], piece, :]
                    span.append(spans[a] + spans[a + 1])
                    merged.append(one + two)
                groups, spans = merged, span
                continue
            partner = (plan.flip(me, bit), core)
            high = (me // bit) % 2 == 1
            for u, g in enumerate(groups):
                if c == 0:
                    sent_log[at + u] = jnp.broadcast_to(spans[u], sent_log.shape[1:])
                    mail_s.send(sent_log.at[at + u], got_log.at[at + u], partner, (CHUNKS + 1) * (at + u))
                sent[at + u, piece, :] = ends[g[0], piece, :].astype(jnp.bfloat16)
                mail_s.send(
                    sent.at[at + u, piece, :], got.at[at + u, piece, :], partner, (CHUNKS + 1) * (at + u) + 1 + c
                )
            yield
            for u, g in enumerate(groups):
                if c == 0:
                    mail_s.receive(got_log.at[at + u], partner, (CHUNKS + 1) * (at + u))
                mail_s.receive(got.at[at + u, piece, :], partner, (CHUNKS + 1) * (at + u) + 1 + c)
                value = got[at + u, piece, :].astype(jnp.float32)
                value_log = got_log[at + u, 0:1, :]
                for i in g:
                    hold[i, piece, :] = hold[i, piece, :] + jnp.where(high, jnp.exp(ahead[i]), 0.0) * value
                    ahead[i] = ahead[i] + jnp.where(high, value_log, 0.0)
                if bit != plan.bits[-1]:
                    ends[g[0], piece, :] = (
                        jnp.exp(jnp.where(high, 0.0, value_log)) * ends[g[0], piece, :]
                        + jnp.exp(jnp.where(high, spans[u], 0.0)) * value
                    )
                    spans[u] = spans[u] + value_log
            at += len(groups)
        for u in range(blocks):
            starts[u, piece, :] = hold[u, piece, :].astype(jnp.bfloat16)
        yield

    scans = [scan(c) for c in range(CHUNKS)]
    steps = len([b for b in plan.bits if b not in plan.team])

    def step_scans():
        for one in scans:
            next(one)

    step_scans()
    cut = (heads + 1) // 2
    if line:
        line_step(mail_o, o_at, 1, 0)
        line_await(mail_q, q_at, (0, 1, -1, 2, -2, 3, -3))
    else:
        own_out(mail_o, o_from, plan.span[::-1])
        for d in range(1, cut):
            forward(mail_o, o_at, 0, d)
        for s in late:
            for d in range(heads):
                await_piece(mail_q, q_at, s, d)

    def queries(index, nothing):
        u = index // per_run
        at = pl.ds(pl.multiple_of(index * tile, tile), tile)
        joined = term(at, spread[0], KV, KV + DK)
        if staged:
            for s in spread[1:]:
                joined = joined + term(at, s, KV, KV + DK)
        joined = joined.astype(jnp.bfloat16).astype(jnp.float32) * DK ** (-0.5)
        past = acc_q[0:1, :]
        past = jnp.where(index % per_run == 0, 0.0, past)
        for b in range(tile // BLOCK):
            here = slice(b * BLOCK, (b + 1) * BLOCK)
            place = pl.ds(pl.multiple_of(index * tile + b * BLOCK, BLOCK), BLOCK)
            q = joined[here]
            k = Kb[place, :].astype(jnp.float32)
            cumul = G[place, :]
            centre = cumul - cumul[BLOCK // 2 : BLOCK // 2 + 1]
            final = cumul[BLOCK - 1 : BLOCK]
            q_scaled = (q * jnp.exp(centre)).astype(jnp.bfloat16)
            k_scaled = (k * jnp.exp(-centre)).astype(jnp.bfloat16)
            scores = lax.dot_general(q_scaled, k_scaled, NT, preferred_element_type=jnp.float32)
            scores = jnp.where(causal, scores, 0.0).astype(jnp.bfloat16)
            near = (q * jnp.exp(cumul)).astype(jnp.bfloat16)
            within[place, :] = jnp.dot(scores, Vb[place, :], preferred_element_type=jnp.float32) + lax.dot_general(
                near, carries[index * (tile // BLOCK) + b], NT, preferred_element_type=jnp.float32
            )
            reach[place, :] = (q * jnp.exp(cumul + past)).astype(jnp.bfloat16)
            past = past + final
        acc_q[0:1, :] = past
        return nothing

    acc_q[...] = jnp.zeros_like(acc_q)
    middle = heads * tiles // 2
    if line:
        for c, one in enumerate(scans):
            lax.fori_loop(middle * c // CHUNKS, middle * (c + 1) // CHUNKS, queries, 0)
            next(one)
    else:
        lax.fori_loop(0, middle, queries, 0)
        if steps:
            step_scans()
    if line:
        line_step(mail_o, o_at, 1, 1)
    else:
        for d in range(max(cut, 1), heads):
            forward(mail_o, o_at, 0, d)
    lax.fori_loop(middle, heads * tiles, queries, 0)
    if line:
        line_step(mail_o, o_at, 2, 0)
        line_step(mail_o, o_at, 2, 1)
    else:
        for s in early:
            if s:
                for d in range(cut):
                    forward(mail_o, o_at, s, d)
    for _ in range(steps - 1):
        step_scans()

    def shape(index, nothing):
        u = index // per_run
        at = pl.ds(pl.multiple_of(index * tile, tile), tile)
        wide = within[at, :] + lax.dot_general(reach[at, :], starts[u], NT, preferred_element_type=jnp.float32)
        value = wide * lax.rsqrt(jnp.mean(wide * wide, axis=-1, keepdims=True) + EPS) * out_gain[...]
        value = value.astype(jnp.bfloat16)
        if tile == seg:
            for c in range(tp):
                to = pl.ds(pl.multiple_of((c * heads + index) * share, share), share)
                shaped[to, :] = value[c * share : (c + 1) * share]
        else:
            for p in range(tile // share):
                lot = index * (tile // share) + p
                to = pl.ds(pl.multiple_of(((lot % tp) * heads + lot // tp) * share, share), share)
                shaped[to, :] = value[p * share : (p + 1) * share]
        return nothing

    lax.fori_loop(0, heads * tiles, shape, 0)

    mail_r = Mail(r_send, r_recv)
    lots = heads * share
    width = out.shape[1]
    groups = [[s] for s in spread] if staged else [spread]
    fields = heads // run

    def product(c, group):
        left = shaped[pl.ds(pl.multiple_of(c * lots, lots), lots), :]
        if staged:
            right = []
            for t in range(fields):
                place = plan.base(plan.flip(me, group[0]), t) * cols
                right.append(WO[0, :, pl.ds(pl.multiple_of(place, run * cols), run * cols)])
            return [jnp.dot(left, one, preferred_element_type=jnp.float32) for one in right]
        if len(WO.shape) == 4:
            return [jnp.dot(left, WO[0, s], preferred_element_type=jnp.float32) for s in range(n)]
        return [jnp.dot(left, WO[0], preferred_element_type=jnp.float32)]

    def spots(values):
        at, result = 0, []
        for value in values:
            result.append(slice(at, at + value.shape[1]))
            at += value.shape[1]
        return result

    per_group = heads * tp + heads
    for g, group in enumerate(groups):
        for s in group:
            if line:
                if g == 1:
                    line_step(mail_o, o_at, 3, 0)
                    line_step(mail_o, o_at, 3, 1)
                if g >= 2:
                    line_await(mail_o, o_at, (0, 1, -1) if g == 2 else (2, -2, 3, -3))
            elif s in late:
                for d in range(heads):
                    await_piece(mail_o, o_at, s, d)
            elif s:
                for d in range(cut, heads):
                    forward(mail_o, o_at, s, d)
        for e, c in enumerate(cores):
            values = product(c, group)
            for place, value in zip(spots(values), values):
                part[g, e, :, place] = value.astype(jnp.bfloat16)
            mail_r.send(part.at[g, e], from_core.at[g, e], (me, c), g * per_group + e)
        values = product(core, group)
        for place, value in zip(spots(values), values):
            total[g, :, place] = value
        for e, c in enumerate(back):
            mail_r.receive(from_core.at[g, e], (me, c), g * per_group + e)
            total[g] = total[g] + from_core[g, e].astype(jnp.float32)
        if heads > 1:
            sum_out[g] = total[g].astype(jnp.bfloat16)
        for d in range(heads - 1, 0, -1):
            lot = pl.ds(pl.multiple_of(plan.member(peers[d]) * share, share), share)
            mail_r.send(sum_out.at[g, lot, :], sum_in.at[g, d - 1], (peers[d], core), g * per_group + heads * tp + d)
    for g, group in enumerate(groups):
        lot = pl.ds(pl.multiple_of(mine * share, share), share)
        value = total[g, lot, :]
        for d in range(heads - 1, 0, -1):
            mail_r.receive(sum_in.at[g, d - 1], (peers[d], core), g * per_group + heads * tp + d)
            value = value + sum_in[g, d - 1].astype(jnp.float32)
        value = value.astype(jnp.bfloat16)
        if staged:
            for t in range(fields):
                place = plan.base(plan.flip(me, group[0]), t) * cols
                out[:, pl.ds(pl.multiple_of(place, run * cols), run * cols)] = value[:, t * run * cols : (t + 1) * run * cols]
        else:
            out[...] = value
    for box in (mail_kv, mail_q, mail_o, mail_x, mail_s, mail_r):
        box.finish()


def on_device(
    tokens, norm_gain, w_query, w_key, w_value, w_rank_down, w_rank_up, gate_bias, decay_shift, out_gain, w_out
):
    n, tp = lax.axis_size("sp"), lax.axis_size("tp")
    heads = w_query.shape[1] // DK
    plan = Plan(n, tp, heads)
    rows, width = tokens.shape
    deep = w_query.shape[0]
    seg = rows * tp
    count = heads * seg
    dma, vmem = pltpu.SemaphoreType.DMA, pltpu.VMEM
    cols = w_out.shape[1]
    aligned = cols % 128 == 0
    staged = aligned and len(plan.span) > 0 and plan.run * deep % 256 == 0
    groups = len(plan.spread) if staged else 1
    field = width // groups
    sides = 2 if plan.line else 1
    posts = 42 if plan.line else n
    most = max(1, plan.blocks * len(plan.span))
    given = max(1, tp - 1)
    bf16, f32 = jnp.bfloat16, jnp.float32
    slots = 80 if plan.line else 2 * n + 8 * (heads + len(plan.span))
    tokens_sent = heads * (tp + 2 + len(plan.team))
    return pl.pallas_call(
        functools.partial(layer_kernel, plan, staged),
        out_shape=jax.ShapeDtypeStruct((rows, width), bf16),
        in_specs=[VMEM] * 11,
        out_specs=VMEM,
        scratch_shapes=[
            vmem((count, width), bf16),
            vmem((heads, 8, seg), f32),
            vmem((sides, n * deep, KV + DK), bf16),
            vmem((sides, DV, n * cols) if aligned else (sides, n, DV, cols), bf16),
            vmem((count, KV) if staged else (8, 128), f32),
            vmem((8, DK), f32),
            vmem((count, DK), f32),
            vmem((count, DK), bf16),
            vmem((count, DV), bf16),
            vmem((count // BLOCK, DV, DK), bf16),
            vmem((count, DV), f32),
            vmem((count, DK), bf16),
            vmem((plan.blocks, DV, DK), f32),
            vmem((plan.blocks, 8, DK), f32),
            vmem((plan.blocks, DV, DK), f32),
            vmem((plan.blocks, DV, DK), bf16),
            vmem((most, DV, DK), bf16),
            vmem((most, DV, DK), bf16),
            vmem((most, 8, DK), f32),
            vmem((most, 8, DK), f32),
            vmem((count, DV), bf16),
            vmem((groups, given, heads * rows, field), bf16),
            vmem((groups, given, heads * rows, field), bf16),
            vmem((groups, heads * rows, field), f32),
            vmem((groups, heads * rows, field) if heads > 1 else (1, 16, 128), bf16),
            vmem((groups, max(1, heads - 1), rows, field) if heads > 1 else (1, 1, 16, 128), bf16),
            dma((slots,)),
            dma((posts,)),
            dma((slots,)),
            dma((posts,)),
            dma((slots,)),
            dma((posts,)),
            dma((tokens_sent,)),
            dma((heads * (tp + 2),)),
            dma(((CHUNKS + 1) * most,)),
            dma(((CHUNKS + 1) * most,)),
            dma((groups * (heads + tp),)),
            dma((groups * (heads * tp + heads),)),
            dma((4,)),
        ],
        compiler_params=pltpu.CompilerParams(
            collective_id=0, has_side_effects=True, vmem_limit_bytes=LIMIT
        ),
        name="layer",
    )(
        tokens,
        norm_gain[None],
        decay_shift[None],
        w_query,
        w_key,
        w_value,
        w_out,
        w_rank_down.T,
        w_rank_up,
        gate_bias[None],
        out_gain[None],
    )


def solution(mesh):
    return jax.shard_map(
        on_device,
        mesh=mesh,
        in_specs=(
            P(("sp", "tp"), None),
            P(),
            P("sp", "tp"),
            P("sp", "tp"),
            P("sp", "tp"),
            P(),
            P(None, "tp"),
            P("tp"),
            P("sp"),
            P(),
            P("tp", "sp"),
        ),
        out_specs=P(("sp", "tp"), None),
        check_vma=False,
    )
```

```python
import functools

import jax
import jax.numpy as jnp
from jax import lax
from jax.experimental import pallas as pl
from jax.experimental.pallas import tpu as pltpu
from jax.sharding import PartitionSpec as P

DK = 256
DV = 512
KV = DK + DV
TAU = 16
BLOCK = 64
EPS = 1e-06
CHUNKS = 4
MESH = pl.DeviceIdType.MESH
VMEM = pl.BlockSpec(memory_space=pltpu.VMEM)
LIMIT = 60 * 2**20
NT = (((1,), (1,)), ((), ()))
TN = (((0,), (0,)), ((), ()))


class Plan:
    def __init__(self, n, tp, heads):
        self.n, self.tp, self.heads = n, tp, heads
        bits = [1 << k for k in range(n.bit_length() - 1)]
        order = [b for b in (1, 4, 2) if b in bits] + [b for b in bits if b > 4]
        self.team = sorted(order[: heads.bit_length() - 1])
        self.span = sorted((b for b in bits if b not in self.team), reverse=True)
        self.bits = bits
        self.run = 1
        while self.run in self.team:
            self.run *= 2
        self.blocks = heads // self.run
        self.line = self.team == [1, 4] and self.span == [8, 2]
        self.spread = [0]
        for b in self.span:
            self.spread = self.spread + [s | b for s in self.spread]

    def mask(self, d):
        return sum(b for k, b in enumerate(self.team) if d >> k & 1)

    def hop(self, s):
        return max((k for k, b in enumerate(self.span) if s & b), default=-1)

    def flip(self, index, mask):
        for b in self.bits:
            if mask & b:
                index = index + b * (1 - 2 * ((index // b) % 2))
        return index

    def member(self, index):
        return sum((((index // b) % 2) << k for k, b in enumerate(self.team)), 0 * index)

    def other(self, member, d):
        for k in range(len(self.team)):
            b = 1 << k
            member = member + b * (1 - 2 * ((member // b) % 2)) * ((d // b) % 2)
        return member

    def base(self, index, t):
        for k, b in enumerate(self.team):
            index = index - b * ((index // b) % 2) + b * (t * self.run >> k & 1)
        return index


def greet(devices, extra, inner):
    barrier = pltpu.get_barrier_semaphore()
    for device in devices:
        pl.semaphore_signal(barrier, inc=1, device_id=device, device_id_type=MESH)
    if extra is None:
        pl.semaphore_wait(barrier, len(devices))
    else:

        @pl.when(inner)
        def _():
            pl.semaphore_signal(barrier, inc=1, device_id=extra, device_id_type=MESH)
            pl.semaphore_wait(barrier, len(devices) + 1)

        @pl.when(jnp.logical_not(inner))
        def _():
            pl.semaphore_wait(barrier, len(devices))


class Mail:
    def __init__(self, send_sem, recv_sem):
        self.send_sem, self.recv_sem, self.out = send_sem, recv_sem, []

    def send(self, src, dst, device, slot, held=False, when=None):
        copy = pltpu.make_async_remote_copy(
            src_ref=src,
            dst_ref=dst,
            send_sem=self.send_sem.at[len(self.out)],
            recv_sem=self.recv_sem.at[slot],
            device_id=device,
            device_id_type=MESH,
        )
        if not held:
            copy.start()
        self.out.append((copy, when))
        return copy

    def receive(self, dst, device, slot):
        pltpu.make_async_remote_copy(
            src_ref=dst,
            dst_ref=dst,
            send_sem=self.send_sem.at[0],
            recv_sem=self.recv_sem.at[slot],
            device_id=device,
            device_id_type=MESH,
        ).wait_recv()

    def finish(self):
        for copy, when in self.out:
            if when is None:
                copy.wait_send()
            else:
                pl.when(when)(copy.wait_send)


def layer_kernel(
    plan, staged, tokens, gain, shift, wq, wk, wv, wo, down, up, bias, out_gain, out,
    X, SH, W, WO, acc_kv, acc_q, G, Kb, Vb, carries, within, reach, ends, logs, hold, starts,
    sent, got, sent_log, got_log, shaped, part, from_core, total, sum_out, sum_in, relay,
    kv_send, kv_recv, q_send, q_recv, o_send, o_recv, x_send, x_recv, s_send, s_recv, r_send, r_recv, local_sem,
):
    n, tp, heads, run, blocks = plan.n, plan.tp, plan.heads, plan.run, plan.blocks
    me, core = lax.axis_index("sp"), lax.axis_index("tp")
    rows, cols = wq.shape[0], wo.shape[1]
    share = tokens.shape[0]
    seg = share * tp
    cores = [lax.rem(core + e, tp) for e in range(1, tp)]
    back = [lax.rem(core + tp - e, tp) for e in range(1, tp)]
    peers = [plan.flip(me, plan.mask(d)) for d in range(heads)]
    mine = plan.member(me)
    last_hop = len(plan.span) - 1
    greet(
        [(p, core) for p in peers[1:]]
        + [(plan.flip(me, b), core) for b in plan.span]
        + [(me, c) for c in cores],
        (plan.flip(me, 12), core) if plan.line else None,
        (me // 4) % 2 != (me // 8) % 2,
    )
    mail_kv, mail_q, mail_o, mail_x = Mail(kv_send, kv_recv), Mail(q_send, q_recv), Mail(o_send, o_recv), Mail(x_send, x_recv)
    base_s, base_c = heads, 2 * heads

    def lines(index):
        return pl.ds(pl.multiple_of(index * rows, rows), rows)

    def kv_at(index, j=0):
        return W.at[j, lines(index), 0:KV]

    def q_at(index, j=0):
        return W.at[j, lines(index), KV:]

    def o_at(index, j=0):
        if len(WO.shape) == 4:
            return WO.at[j, index]
        return WO.at[j, :, pl.ds(pl.multiple_of(index * cols, cols), cols)]

    def kv_from(m, j=0):
        place = lines(me)
        return [
            (wk.at[:, pl.ds(pl.multiple_of(m * DK, DK), DK)], W.at[j, place, 0:DK]),
            (wv.at[:, pl.ds(pl.multiple_of(m * DV, DV), DV)], W.at[j, place, DK:KV]),
        ]

    def q_from(m, j=0):
        return [(wq.at[:, pl.ds(pl.multiple_of(m * DK, DK), DK)], W.at[j, lines(me), KV:])]

    def o_from(m, j=0):
        return [(wo.at[pl.ds(pl.multiple_of(m * DV, DV), DV), :], o_at(me, j))]

    plane = me // 4
    y_peer = (plan.flip(me, 2), core)

    def tag(dz, q, kind):
        return ((dz + 3) * 2 + q) * 3 + kind

    def source(dz, q, y):
        return plan.flip(me, q + 2 * y) + 4 * dz

    def room(sign):
        return (3 - plane, plane) if sign > 0 else (plane, 3 - plane)

    def line_open(box, pairs):
        for j in (0, 1):
            for src, dst in pairs(plan.other(mine, 1 + 2 * j), j):
                box.send(src, dst, (peers[1], core), tag(0, 1, j))

    def line_own_y(box, pairs):
        for src, dst in pairs(mine, 0):
            box.send(src, dst, y_peer, tag(0, 0, 2))

    def line_own_z(box, pairs):
        for j in (1, 0):
            for sign in (1, -1):
                test = room(sign)[0] >= 2 - j
                copies = [
                    box.send(src, dst, (me + 4 * sign, core), tag(-sign, 0, 1 - j), True, test)
                    for src, dst in pairs(plan.other(mine, 2 * j), 1 - j)
                ]
                start_if(test, copies)

    def line_x_y(box, view):
        for j in (0, 1):
            index = source(0, 1, 0)
            box.receive(view(index, j), (peers[1], core), tag(0, 1, j))
            if j == 0:
                box.send(view(index), view(index), y_peer, tag(0, 1, 2))

    def line_x_z(box, view):
        index = source(0, 1, 0)
        for j in (0, 1):
            for sign in (1, -1):
                test = room(sign)[0] >= 2 - j
                start_if(test, [
                    box.send(view(index, j), view(index, 1 - j), (me + 4 * sign, core), tag(-sign, 1, 1 - j), True, test)
                ])

    def line_step(box, view, k, q):
        for sign in (1, -1):
            ahead, behind = room(sign)
            for j in (0, 1):
                if k + j > 3:
                    continue
                index = source(-sign * k, q, 0)
                test = (behind >= k) & (ahead >= j)
                onward = (behind >= k) & (ahead >= 2 - j)
                over = [box.send(view(index), view(index), y_peer, tag(-sign * k, q, 2), True, test)] if j == 0 else []
                on = []
                if k + 2 - j <= 3:
                    on.append(
                        box.send(
                            view(index, j), view(index, 1 - j), (me + 4 * sign, core),
                            tag(-sign * (k + 1), q, 1 - j), True, onward,
                        )
                    )

                @pl.when(test)
                def _():
                    box.receive(view(index, j), (me - 4 * sign, core), tag(-sign * k, q, j))
                    for copy in over:
                        copy.start()

                if on:
                    start_if(onward, on)

    def line_await(box, view, gaps):
        for dz in gaps:
            for q in (0, 1):
                test = (plane + dz >= 0) & (plane + dz <= 3)

                @pl.when(test)
                def _():
                    box.receive(view(source(dz, q, 1)), y_peer, tag(dz, q, 2))

    def to_team(box, pairs):
        for d in range(1, heads):
            for src, dst in pairs(plan.member(peers[d])):
                box.send(src, dst, (peers[d], core), plan.mask(d))

    def own_out(box, pairs, bits, held=False):
        return [
            box.send(src, dst, (plan.flip(me, b), core), b, held) for b in bits for src, dst in pairs(mine)
        ]

    def start_if(test, copies):
        @pl.when(test)
        def _():
            for copy in copies:
                copy.start()

    def await_piece(box, view, s, d):
        if s == 0 and d == 0:
            return
        mask = s | plan.mask(d)
        hop = plan.hop(s)
        sender = peers[d] if hop < 0 else plan.flip(me, plan.span[hop])
        box.receive(view(plan.flip(me, mask)), (sender, core), mask)

    def hand_over(box, view, s, d):
        mask = s | plan.mask(d)
        source = plan.flip(me, mask)
        for later in range(plan.hop(s) + 1, last_hop + 1):
            bit = plan.span[later]
            box.send(view(source), view(source), (plan.flip(me, bit), core), mask ^ bit)

    def forward(box, view, s, d):
        await_piece(box, view, s, d)
        hand_over(box, view, s, d)

    def slot_rows(member, c):
        return pl.ds(pl.multiple_of((member * tp + c) * share, share), share)

    def slot(index, c):
        return X.at[slot_rows(plan.member(index), c), :]

    locals_ = []
    for at, (src, dst) in enumerate(kv_from(mine) + q_from(mine) + o_from(mine)):
        copy = pltpu.make_async_copy(src, dst, local_sem.at[at])
        copy.start()
        locals_.append(copy)
    line = plan.line
    if line:
        line_open(mail_kv, kv_from)
        line_own_y(mail_kv, kv_from)
        line_own_z(mail_kv, kv_from)
        line_open(mail_q, q_from)
        line_own_y(mail_q, q_from)
    else:
        to_team(mail_kv, kv_from)
        own_out(mail_kv, kv_from, plan.span)
        to_team(mail_q, q_from)
        own_out(mail_q, q_from, plan.span)
    raw = tokens[...].astype(jnp.float32)
    raw = raw * lax.rsqrt(jnp.mean(raw * raw, axis=-1, keepdims=True) + EPS) * gain[...]
    X[slot_rows(mine, core), :] = raw.astype(jnp.bfloat16)
    SH[mine] = jnp.broadcast_to(shift[...], SH.shape[1:])

    def token_on(d, top):
        for k in range(top):
            mail_x.send(slot(peers[d], core), slot(peers[d], core), (peers[1 << k], core), d ^ (1 << k))
        for e, c in enumerate(cores):
            mail_x.send(slot(peers[d], core), slot(peers[d], core), (me, c), base_c + d * (tp - 1) + e)

    def token_in(d):
        k = d.bit_length() - 1
        low = (d & -d).bit_length() - 1
        mail_x.receive(slot(peers[d], core), (peers[1 << low], core), d)
        token_on(d, low)

    def token_ready(d):
        for e, c in enumerate(back):
            mail_x.receive(slot(peers[d], c), (me, c), base_c + d * (tp - 1) + e)
        if d:
            mail_x.receive(SH.at[plan.member(peers[d])], (peers[d], core), base_s + d)

    token_on(0, len(plan.team))
    for d in range(1, heads):
        mail_x.send(SH.at[mine], SH.at[mine], (peers[d], core), base_s + d)
    for copy in locals_:
        copy.wait()

    tile = min(seg, 256)
    tiles = seg // tile
    row = lax.broadcasted_iota(jnp.int32, (tile, tile), 0)
    col = lax.broadcasted_iota(jnp.int32, (tile, tile), 1)
    lower = (row >= col) & (row // BLOCK == col // BLOCK)
    ones = jnp.where(lower, 1.0, 0.0).astype(jnp.bfloat16)
    causal = lax.broadcasted_iota(jnp.int32, (BLOCK, BLOCK), 0) >= lax.broadcasted_iota(jnp.int32, (BLOCK, BLOCK), 1)
    up_here = up[:, pl.ds(pl.multiple_of(mine * DK, DK), DK)]
    bias_here = bias[:, pl.ds(pl.multiple_of(mine * DK, DK), DK)]

    def gates(d, t):
        i = plan.other(mine, d)
        at = pl.ds(pl.multiple_of(i * seg + t * tile, tile), tile)
        rank = lax.dot_general(X[at, :], down[...], NT, preferred_element_type=jnp.float32)
        pre = jnp.dot(rank.astype(jnp.bfloat16), up_here, preferred_element_type=jnp.float32) + bias_here
        gate = (jnp.minimum(pre, 0.0) - jnp.log1p(jnp.exp(-jnp.abs(pre)))) / TAU
        moved = SH[i, 0:1, pl.ds(pl.multiple_of(t * tile, tile), tile)]
        first = gate.astype(jnp.bfloat16)
        rest = gate - first.astype(jnp.float32)
        second = rest.astype(jnp.bfloat16)
        third = (rest - second.astype(jnp.float32)).astype(jnp.bfloat16)
        G[at, :] = (
            jnp.dot(ones, first, preferred_element_type=jnp.float32)
            + jnp.dot(ones, second, preferred_element_type=jnp.float32)
            + jnp.dot(ones, third, preferred_element_type=jnp.float32)
            + jnp.sum(jnp.where(lower, moved, 0.0), axis=1, keepdims=True)
        )

    def gates_of(low, high):
        def body(step, nothing):
            gates(low + step // tiles, step % tiles)
            return nothing

        lax.fori_loop(0, (high - low) * tiles, body, 0)

    def term(at, s, lo, hi):
        if staged:
            value = None
            for t in range(heads // run):
                place = plan.base(plan.flip(me, s), t) * rows
                span = pl.ds(pl.multiple_of(place, rows * run), rows * run)
                one = jnp.dot(X[at, span], W[0, span, lo:hi], preferred_element_type=jnp.float32)
                value = one if value is None else value + one
            return value
        return jnp.dot(X[at, :], W[0, :, lo:hi], preferred_element_type=jnp.float32)

    def accumulate(acc, lo, hi, s, first, low, high):
        def body(step, nothing):
            i = plan.other(mine, low + step // tiles)
            at = pl.ds(pl.multiple_of(i * seg + (step % tiles) * tile, tile), tile)
            value = term(at, s, lo, hi)
            acc[at, :] = value if first else acc[at, :] + value
            return nothing

        lax.fori_loop(0, (high - low) * tiles, body, 0)

    spread = plan.spread
    early = [s for s in spread if not s or plan.hop(s) < last_hop]
    late = [s for s in spread if s not in early]
    solo = [1 << k for k in range(len(plan.team))]
    rest = [d for d in range(1, heads) if d not in solo]
    waiting = [(s, d) for s in early if s for d in range(heads)]
    if line:
        line_x_y(mail_kv, kv_at)
        line_x_z(mail_kv, kv_at)
        line_step(mail_kv, kv_at, 1, 0)
        token_ready(0)
        gates_of(0, 1)
        line_x_y(mail_q, q_at)
        line_own_y(mail_o, o_from)
        for d in solo:
            token_in(d)
        line_step(mail_kv, kv_at, 1, 1)
        line_open(mail_o, o_from)
        token_ready(1)
        gates_of(1, 2)
        line_step(mail_kv, kv_at, 2, 0)
        token_ready(2)
        gates_of(2, 3)
        line_step(mail_kv, kv_at, 2, 1)
        line_own_z(mail_q, q_from)
        line_x_z(mail_q, q_at)
        token_in(3)
        accumulate(acc_kv, 0, KV, spread[0], True, 0, 3)
        line_step(mail_kv, kv_at, 3, 0)
        token_ready(3)
        gates_of(3, 4)
        accumulate(acc_kv, 0, KV, spread[0], True, 3, 4)
        line_step(mail_kv, kv_at, 3, 1)
        line_step(mail_q, q_at, 1, 0)
        line_step(mail_q, q_at, 1, 1)
        accumulate(acc_kv, 0, KV, spread[1], False, 0, heads)
        line_await(mail_kv, kv_at, (0, 1, -1))
        line_step(mail_q, q_at, 2, 0)
        line_step(mail_q, q_at, 2, 1)
        line_own_z(mail_o, o_from)
        line_x_y(mail_o, o_at)
        line_x_z(mail_o, o_at)
        accumulate(acc_kv, 0, KV, spread[2], False, 0, heads)
        line_step(mail_q, q_at, 3, 0)
        line_step(mail_q, q_at, 3, 1)
        line_await(mail_kv, kv_at, (2, -2, 3, -3))
    else:
        for d in range(1, heads):
            forward(mail_kv, kv_at, 0, d)
        token_ready(0)
        gates_of(0, 1)
        for d in range(1, heads):
            forward(mail_q, q_at, 0, d)
        to_team(mail_o, o_from)
        for d in solo:
            token_in(d)
        for d in solo:
            token_ready(d)
            gates_of(d, d + 1)
        for s, e in waiting:
            forward(mail_kv, kv_at, s, e)
    if not line:
        near_heads = 3 if heads > 2 else heads
        for d in rest:
            token_in(d)
        if staged:
            for at, s in enumerate(spread[:-1]):
                if s in late:
                    for d in range(heads):
                        await_piece(mail_kv, kv_at, s, d)
                accumulate(acc_kv, 0, KV, s, at == 0, 0, near_heads)
        for d in rest:
            token_ready(d)
            gates_of(d, d + 1)
        for s, e in waiting:
            forward(mail_q, q_at, s, e)
        if staged:
            for at, s in enumerate(spread[:-1]):
                accumulate(acc_kv, 0, KV, s, at == 0, near_heads, heads)
            for d in range(heads):
                await_piece(mail_kv, kv_at, spread[-1], d)
        else:
            for s in late:
                for d in range(heads):
                    await_piece(mail_kv, kv_at, s, d)

    per_run = run * tiles
    ends[...] = jnp.zeros_like(ends)
    logs[...] = jnp.zeros_like(logs)

    def keys(index, nothing):
        u = index // per_run
        at = pl.ds(pl.multiple_of(index * tile, tile), tile)
        joined = term(at, spread[-1], 0, KV)
        if staged:
            joined = joined + acc_kv[at, :]
        joined = joined.astype(jnp.bfloat16)
        Kb[at, :] = joined[:, :DK]
        Vb[at, :] = joined[:, DK:]
        carry, past = ends[u], logs[u, 0:1, :]
        for b in range(tile // BLOCK):
            here = slice(b * BLOCK, (b + 1) * BLOCK)
            place = pl.ds(pl.multiple_of(index * tile + b * BLOCK, BLOCK), BLOCK)
            cumul = G[place, :]
            final = cumul[BLOCK - 1 : BLOCK]
            carries[index * (tile // BLOCK) + b] = carry.astype(jnp.bfloat16)
            decayed = (joined[here, :DK].astype(jnp.float32) * jnp.exp(final - cumul)).astype(jnp.bfloat16)
            carry = jnp.exp(final) * carry + lax.dot_general(
                joined[here, DK:], decayed, TN, preferred_element_type=jnp.float32
            )
            past = past + final
        ends[u] = carry
        logs[u] = jnp.broadcast_to(past, logs.shape[1:])
        return nothing

    lax.fori_loop(0, heads * tiles, keys, 0)

    mail_s = Mail(s_send, s_recv)
    depth = DV // CHUNKS

    def scan(c):
        piece = slice(c * depth, (c + 1) * depth)
        ahead = [jnp.zeros((1, DK), jnp.float32)] * blocks
        spans = [logs[u, 0:1, :] for u in range(blocks)]
        groups = [[u] for u in range(blocks)]
        for u in range(blocks):
            hold[u, piece, :] = jnp.zeros((depth, DK), jnp.float32)
        at = 0
        for bit in plan.bits:
            if bit < run:
                continue
            if bit in plan.team:
                merged, span = [], []
                for a in range(0, len(groups), 2):
                    one, two = groups[a], groups[a + 1]
                    value = ends[one[0], piece, :]
                    for i in two:
                        hold[i, piece, :] = hold[i, piece, :] + jnp.exp(ahead[i]) * value
                        ahead[i] = ahead[i] + spans[a]
                    ends[one[0], piece, :] = jnp.exp(spans[a + 1]) * value + ends[two[0], piece, :]
                    span.append(spans[a] + spans[a + 1])
                    merged.append(one + two)
                groups, spans = merged, span
                continue
            partner = (plan.flip(me, bit), core)
            high = (me // bit) % 2 == 1
            final = bit == plan.bits[-1]
            low = jnp.logical_not(high) if final else None
            for u, g in enumerate(groups):
                if c == 0:
                    sent_log[at + u] = jnp.broadcast_to(spans[u], sent_log.shape[1:])
                    mail_s.send(
                        sent_log.at[at + u], got_log.at[at + u], partner, (CHUNKS + 1) * (at + u), final, low
                    )
                    if final:
                        start_if(low, [mail_s.out[-1][0]])
                sent[at + u, piece, :] = ends[g[0], piece, :].astype(jnp.bfloat16)
                mail_s.send(
                    sent.at[at + u, piece, :], got.at[at + u, piece, :], partner, (CHUNKS + 1) * (at + u) + 1 + c,
                    final, low,
                )
                if final:
                    start_if(low, [mail_s.out[-1][0]])
            yield
            if final:

                @pl.when(high)
                def _():
                    for u, g in enumerate(groups):
                        if c == 0:
                            mail_s.receive(got_log.at[at + u], partner, (CHUNKS + 1) * (at + u))
                        mail_s.receive(got.at[at + u, piece, :], partner, (CHUNKS + 1) * (at + u) + 1 + c)
                        value = got[at + u, piece, :].astype(jnp.float32)
                        for i in g:
                            hold[i, piece, :] = hold[i, piece, :] + jnp.exp(ahead[i]) * value

                continue
            for u, g in enumerate(groups):
                if c == 0:
                    mail_s.receive(got_log.at[at + u], partner, (CHUNKS + 1) * (at + u))
                mail_s.receive(got.at[at + u, piece, :], partner, (CHUNKS + 1) * (at + u) + 1 + c)
                value = got[at + u, piece, :].astype(jnp.float32)
                value_log = got_log[at + u, 0:1, :]
                for i in g:
                    hold[i, piece, :] = hold[i, piece, :] + jnp.where(high, jnp.exp(ahead[i]), 0.0) * value
                    ahead[i] = ahead[i] + jnp.where(high, value_log, 0.0)
                ends[g[0], piece, :] = (
                    jnp.exp(jnp.where(high, 0.0, value_log)) * ends[g[0], piece, :]
                    + jnp.exp(jnp.where(high, spans[u], 0.0)) * value
                )
                spans[u] = spans[u] + value_log
            at += len(groups)
        for u in range(blocks):
            starts[u, piece, :] = hold[u, piece, :].astype(jnp.bfloat16)
        yield

    scans = [scan(c) for c in range(CHUNKS)]
    steps = len([b for b in plan.bits if b not in plan.team])

    def step_scans():
        for one in scans:
            next(one)

    step_scans()
    cut = (heads + 1) // 2
    if line:
        line_step(mail_o, o_at, 1, 0)
    else:
        own_out(mail_o, o_from, plan.span[::-1])
        for d in range(1, cut):
            forward(mail_o, o_at, 0, d)
        for s in late:
            for d in range(heads):
                await_piece(mail_q, q_at, s, d)

    def queries(index, nothing):
        u = index // per_run
        at = pl.ds(pl.multiple_of(index * tile, tile), tile)
        joined = term(at, spread[0], KV, KV + DK)
        if staged:
            for s in spread[1:]:
                joined = joined + term(at, s, KV, KV + DK)
        joined = joined.astype(jnp.bfloat16).astype(jnp.float32) * DK ** (-0.5)
        past = acc_q[0:1, :]
        past = jnp.where(index % per_run == 0, 0.0, past)
        for b in range(tile // BLOCK):
            here = slice(b * BLOCK, (b + 1) * BLOCK)
            place = pl.ds(pl.multiple_of(index * tile + b * BLOCK, BLOCK), BLOCK)
            q = joined[here]
            k = Kb[place, :].astype(jnp.float32)
            cumul = G[place, :]
            centre = cumul - cumul[BLOCK // 2 : BLOCK // 2 + 1]
            final = cumul[BLOCK - 1 : BLOCK]
            q_scaled = (q * jnp.exp(centre)).astype(jnp.bfloat16)
            k_scaled = (k * jnp.exp(-centre)).astype(jnp.bfloat16)
            scores = lax.dot_general(q_scaled, k_scaled, NT, preferred_element_type=jnp.float32)
            scores = jnp.where(causal, scores, 0.0).astype(jnp.bfloat16)
            near = (q * jnp.exp(cumul)).astype(jnp.bfloat16)
            within[place, :] = jnp.dot(scores, Vb[place, :], preferred_element_type=jnp.float32) + lax.dot_general(
                near, carries[index * (tile // BLOCK) + b], NT, preferred_element_type=jnp.float32
            )
            reach[place, :] = (q * jnp.exp(cumul + past)).astype(jnp.bfloat16)
            past = past + final
        acc_q[0:1, :] = past
        return nothing

    acc_q[...] = jnp.zeros_like(acc_q)
    middle = heads * tiles // 2
    if line:
        for c, one in enumerate(scans):
            next(one)
    else:
        lax.fori_loop(0, middle, queries, 0)
        if steps:
            step_scans()
    if line:
        line_step(mail_o, o_at, 1, 1)
        line_await(mail_q, q_at, (0, 1, -1, 2, -2, 3, -3))
    else:
        for d in range(max(cut, 1), heads):
            forward(mail_o, o_at, 0, d)
    lax.fori_loop(0 if line else middle, heads * tiles, queries, 0)
    if line:
        line_step(mail_o, o_at, 2, 0)
        line_step(mail_o, o_at, 2, 1)
    else:
        for s in early:
            if s:
                for d in range(cut):
                    forward(mail_o, o_at, s, d)
    for _ in range(steps - 1):
        step_scans()

    def shape(index, nothing):
        u = index // per_run
        at = pl.ds(pl.multiple_of(index * tile, tile), tile)
        wide = within[at, :] + lax.dot_general(reach[at, :], starts[u], NT, preferred_element_type=jnp.float32)
        value = wide * lax.rsqrt(jnp.mean(wide * wide, axis=-1, keepdims=True) + EPS) * out_gain[...]
        value = value.astype(jnp.bfloat16)
        if tile == seg:
            for c in range(tp):
                to = pl.ds(pl.multiple_of((c * heads + index) * share, share), share)
                shaped[to, :] = value[c * share : (c + 1) * share]
        else:
            for p in range(tile // share):
                lot = index * (tile // share) + p
                to = pl.ds(pl.multiple_of(((lot % tp) * heads + lot // tp) * share, share), share)
                shaped[to, :] = value[p * share : (p + 1) * share]
        return nothing

    lax.fori_loop(0, heads * tiles, shape, 0)

    mail_r = Mail(r_send, r_recv)
    lots = heads * share
    width = out.shape[1]
    groups = [[s] for s in spread] if staged else [spread]
    fields = heads // run

    def product(c, group):
        left = shaped[pl.ds(pl.multiple_of(c * lots, lots), lots), :]
        if staged:
            right = []
            for t in range(fields):
                place = plan.base(plan.flip(me, group[0]), t) * cols
                right.append(WO[0, :, pl.ds(pl.multiple_of(place, run * cols), run * cols)])
            return [jnp.dot(left, one, preferred_element_type=jnp.float32) for one in right]
        if len(WO.shape) == 4:
            return [jnp.dot(left, WO[0, s], preferred_element_type=jnp.float32) for s in range(n)]
        return [jnp.dot(left, WO[0], preferred_element_type=jnp.float32)]

    def spots(values):
        at, result = 0, []
        for value in values:
            result.append(slice(at, at + value.shape[1]))
            at += value.shape[1]
        return result

    per_group = heads * tp + heads

    def lot_of(d):
        return pl.ds(pl.multiple_of(plan.member(peers[d]) * share, share), share)

    def for_others(g):
        for e, c in enumerate(cores):
            values = product(c, groups[g])
            for place, value in zip(spots(values), values):
                part[g, e, :, place] = value.astype(jnp.bfloat16)
            mail_r.send(part.at[g, e], from_core.at[g, e], (me, c), g * per_group + e)

    def for_self(g):
        values = product(core, groups[g])
        for place, value in zip(spots(values), values):
            total[g, :, place] = value

    def add_cores(g):
        for e, c in enumerate(back):
            mail_r.receive(from_core.at[g, e], (me, c), g * per_group + e)
            total[g] = total[g] + from_core[g, e].astype(jnp.float32)
        if heads > 1:
            sum_out[g] = total[g].astype(jnp.bfloat16)

    def place_out(g, value):
        if staged:
            for t in range(fields):
                place = plan.base(plan.flip(me, groups[g][0]), t) * cols
                out[:, pl.ds(pl.multiple_of(place, run * cols), run * cols)] = value[:, t * run * cols : (t + 1) * run * cols]
        else:
            out[...] = value

    if line:
        half = out.shape[1] // len(groups) // 2
        sides = [slice(0, half), slice(half, 2 * half)]

        def pass_far(g):
            for d in (1, 2):
                mail_r.send(
                    sum_out.at[g, lot_of(3), sides[d - 1]], relay.at[g, d - 1], (peers[d], core), g * per_group + tp + d
                )

        def send_near(g):
            for d in (1, 2):
                mail_r.receive(relay.at[g, d - 1], (peers[d], core), g * per_group + tp + d)
                to = lot_of(3 - d)
                sum_out[g, to, sides[d - 1]] = (
                    total[g, to, sides[d - 1]] + relay[g, d - 1].astype(jnp.float32)
                ).astype(jnp.bfloat16)
                mail_r.send(
                    sum_out.at[g, to, :], sum_in.at[g, 2 - d], (peers[3 - d], core), g * per_group + tp + 5 - d
                )

        for_others(0)
        for_self(0)
        line_step(mail_o, o_at, 3, 0)
        line_step(mail_o, o_at, 3, 1)
        for_others(1)
        add_cores(0)
        pass_far(0)
        for_self(1)
        add_cores(1)
        pass_far(1)
        send_near(0)
        line_await(mail_o, o_at, (0, 1, -1))
        for_others(2)
        send_near(1)
        for_self(2)
        add_cores(2)
        pass_far(2)
        line_await(mail_o, o_at, (2, -2, 3, -3))
        for_others(3)
        send_near(2)
        for_self(3)
        add_cores(3)
        pass_far(3)
        send_near(3)
        for g in range(len(groups)):
            value = total[g, lot_of(0), :]
            for d in (1, 2):
                mail_r.receive(sum_in.at[g, d - 1], (peers[d], core), g * per_group + tp + 2 + d)
                value = value + sum_in[g, d - 1].astype(jnp.float32)
            place_out(g, value.astype(jnp.bfloat16))
    else:
        for g, group in enumerate(groups):
            for s in group:
                if s in late:
                    for d in range(heads):
                        await_piece(mail_o, o_at, s, d)
                elif s:
                    for d in range(cut, heads):
                        forward(mail_o, o_at, s, d)
            for_others(g)
            for_self(g)
            add_cores(g)
            for d in range(heads - 1, 0, -1):
                mail_r.send(
                    sum_out.at[g, lot_of(d), :], sum_in.at[g, d - 1], (peers[d], core), g * per_group + heads * tp + d
                )
        for g in range(len(groups)):
            value = total[g, lot_of(0), :]
            for d in range(heads - 1, 0, -1):
                mail_r.receive(sum_in.at[g, d - 1], (peers[d], core), g * per_group + heads * tp + d)
                value = value + sum_in[g, d - 1].astype(jnp.float32)
            place_out(g, value.astype(jnp.bfloat16))
    for box in (mail_kv, mail_q, mail_o, mail_x, mail_s, mail_r):
        box.finish()


def on_device(
    tokens, norm_gain, w_query, w_key, w_value, w_rank_down, w_rank_up, gate_bias, decay_shift, out_gain, w_out
):
    n, tp = lax.axis_size("sp"), lax.axis_size("tp")
    heads = w_query.shape[1] // DK
    plan = Plan(n, tp, heads)
    rows, width = tokens.shape
    deep = w_query.shape[0]
    seg = rows * tp
    count = heads * seg
    dma, vmem = pltpu.SemaphoreType.DMA, pltpu.VMEM
    cols = w_out.shape[1]
    aligned = cols % 128 == 0
    staged = aligned and len(plan.span) > 0 and plan.run * deep % 256 == 0
    groups = len(plan.spread) if staged else 1
    field = width // groups
    sides = 2 if plan.line else 1
    posts = 42 if plan.line else n
    most = max(1, plan.blocks * len(plan.span))
    given = max(1, tp - 1)
    bf16, f32 = jnp.bfloat16, jnp.float32
    slots = 80 if plan.line else 2 * n + 8 * (heads + len(plan.span))
    tokens_sent = heads * (tp + 2 + len(plan.team))
    return pl.pallas_call(
        functools.partial(layer_kernel, plan, staged),
        out_shape=jax.ShapeDtypeStruct((rows, width), bf16),
        in_specs=[VMEM] * 11,
        out_specs=VMEM,
        scratch_shapes=[
            vmem((count, width), bf16),
            vmem((heads, 8, seg), f32),
            vmem((sides, n * deep, KV + DK), bf16),
            vmem((sides, DV, n * cols) if aligned else (sides, n, DV, cols), bf16),
            vmem((count, KV) if staged else (8, 128), f32),
            vmem((8, DK), f32),
            vmem((count, DK), f32),
            vmem((count, DK), bf16),
            vmem((count, DV), bf16),
            vmem((count // BLOCK, DV, DK), bf16),
            vmem((count, DV), f32),
            vmem((count, DK), bf16),
            vmem((plan.blocks, DV, DK), f32),
            vmem((plan.blocks, 8, DK), f32),
            vmem((plan.blocks, DV, DK), f32),
            vmem((plan.blocks, DV, DK), bf16),
            vmem((most, DV, DK), bf16),
            vmem((most, DV, DK), bf16),
            vmem((most, 8, DK), f32),
            vmem((most, 8, DK), f32),
            vmem((count, DV), bf16),
            vmem((groups, given, heads * rows, field), bf16),
            vmem((groups, given, heads * rows, field), bf16),
            vmem((groups, heads * rows, field), f32),
            vmem((groups, heads * rows, field) if heads > 1 else (1, 16, 128), bf16),
            vmem((groups, max(1, heads - 1), rows, field) if heads > 1 else (1, 1, 16, 128), bf16),
            vmem((groups, 2, rows, field // 2) if plan.line else (1, 1, 16, 128), bf16),
            dma((slots,)),
            dma((posts,)),
            dma((slots,)),
            dma((posts,)),
            dma((slots,)),
            dma((posts,)),
            dma((tokens_sent,)),
            dma((heads * (tp + 2),)),
            dma(((CHUNKS + 1) * most,)),
            dma(((CHUNKS + 1) * most,)),
            dma((groups * (heads + tp),)),
            dma((groups * (heads * tp + heads),)),
            dma((4,)),
        ],
        compiler_params=pltpu.CompilerParams(
            collective_id=0, has_side_effects=True, vmem_limit_bytes=LIMIT
        ),
        name="layer",
    )(
        tokens,
        norm_gain[None],
        decay_shift[None],
        w_query,
        w_key,
        w_value,
        w_out,
        w_rank_down.T,
        w_rank_up,
        gate_bias[None],
        out_gain[None],
    )


def solution(mesh):
    return jax.shard_map(
        on_device,
        mesh=mesh,
        in_specs=(
            P(("sp", "tp"), None),
            P(),
            P("sp", "tp"),
            P("sp", "tp"),
            P("sp", "tp"),
            P(),
            P(None, "tp"),
            P("tp"),
            P("sp"),
            P(),
            P("tp", "sp"),
        ),
        out_specs=P(("sp", "tp"), None),
        check_vma=False,
    )
```

```python
import functools

import jax
import jax.numpy as jnp
from jax import lax
from jax.experimental import pallas as pl
from jax.experimental.pallas import tpu as pltpu
from jax.sharding import PartitionSpec as P

DK = 256
DV = 512
KV = DK + DV
TAU = 16
BLOCK = 64
EPS = 1e-06
CHUNKS = 2
MESH = pl.DeviceIdType.MESH
VMEM = pl.BlockSpec(memory_space=pltpu.VMEM)
LIMIT = 60 * 2**20
NT = (((1,), (1,)), ((), ()))
TN = (((0,), (0,)), ((), ()))


class Plan:
    def __init__(self, n, tp, heads):
        self.n, self.tp, self.heads = n, tp, heads
        bits = [1 << k for k in range(n.bit_length() - 1)]
        order = [b for b in (1, 4, 2) if b in bits] + [b for b in bits if b > 4]
        self.team = sorted(order[: heads.bit_length() - 1])
        self.span = sorted((b for b in bits if b not in self.team), reverse=True)
        self.bits = bits
        self.run = 1
        while self.run in self.team:
            self.run *= 2
        self.blocks = heads // self.run
        self.line = self.team == [1, 4] and self.span == [8, 2]
        self.spread = [0]
        for b in self.span:
            self.spread = self.spread + [s | b for s in self.spread]

    def mask(self, d):
        return sum(b for k, b in enumerate(self.team) if d >> k & 1)

    def hop(self, s):
        return max((k for k, b in enumerate(self.span) if s & b), default=-1)

    def flip(self, index, mask):
        for b in self.bits:
            if mask & b:
                index = index + b * (1 - 2 * ((index // b) % 2))
        return index

    def member(self, index):
        return sum((((index // b) % 2) << k for k, b in enumerate(self.team)), 0 * index)

    def other(self, member, d):
        for k in range(len(self.team)):
            b = 1 << k
            member = member + b * (1 - 2 * ((member // b) % 2)) * ((d // b) % 2)
        return member

    def base(self, index, t):
        for k, b in enumerate(self.team):
            index = index - b * ((index // b) % 2) + b * (t * self.run >> k & 1)
        return index


def greet(devices, extra, inner):
    barrier = pltpu.get_barrier_semaphore()
    for device in devices:
        pl.semaphore_signal(barrier, inc=1, device_id=device, device_id_type=MESH)
    if extra is None:
        pl.semaphore_wait(barrier, len(devices))
    else:

        @pl.when(inner)
        def _():
            pl.semaphore_signal(barrier, inc=1, device_id=extra, device_id_type=MESH)
            pl.semaphore_wait(barrier, len(devices) + 1)

        @pl.when(jnp.logical_not(inner))
        def _():
            pl.semaphore_wait(barrier, len(devices))


class Mail:
    def __init__(self, send_sem, recv_sem):
        self.send_sem, self.recv_sem, self.out = send_sem, recv_sem, []

    def send(self, src, dst, device, slot, held=False, when=None):
        copy = pltpu.make_async_remote_copy(
            src_ref=src,
            dst_ref=dst,
            send_sem=self.send_sem.at[len(self.out)],
            recv_sem=self.recv_sem.at[slot],
            device_id=device,
            device_id_type=MESH,
        )
        if not held:
            copy.start()
        self.out.append((copy, when))
        return copy

    def receive(self, dst, device, slot):
        pltpu.make_async_remote_copy(
            src_ref=dst,
            dst_ref=dst,
            send_sem=self.send_sem.at[0],
            recv_sem=self.recv_sem.at[slot],
            device_id=device,
            device_id_type=MESH,
        ).wait_recv()

    def finish(self):
        for copy, when in self.out:
            if when is None:
                copy.wait_send()
            else:
                pl.when(when)(copy.wait_send)


def layer_kernel(
    plan, staged, tokens, gain, shift, wq, wk, wv, wo, down, up, bias, out_gain, out,
    X, SH, W, WO, acc_kv, acc_q, G, Kb, Vb, carries, within, reach, ends, logs, hold, starts,
    sent, got, sent_log, got_log, shaped, part, from_core, total, sum_out, sum_in, relay,
    kv_send, kv_recv, q_send, q_recv, o_send, o_recv, x_send, x_recv, s_send, s_recv, r_send, r_recv, local_sem,
):
    n, tp, heads, run, blocks = plan.n, plan.tp, plan.heads, plan.run, plan.blocks
    me, core = lax.axis_index("sp"), lax.axis_index("tp")
    rows, cols = wq.shape[0], wo.shape[1]
    share = tokens.shape[0]
    seg = share * tp
    cores = [lax.rem(core + e, tp) for e in range(1, tp)]
    back = [lax.rem(core + tp - e, tp) for e in range(1, tp)]
    peers = [plan.flip(me, plan.mask(d)) for d in range(heads)]
    mine = plan.member(me)
    last_hop = len(plan.span) - 1
    greet(
        [(p, core) for p in peers[1:]]
        + [(plan.flip(me, b), core) for b in plan.span]
        + [(me, c) for c in cores],
        (plan.flip(me, 12), core) if plan.line else None,
        (me // 4) % 2 != (me // 8) % 2,
    )
    mail_kv, mail_q, mail_o, mail_x = Mail(kv_send, kv_recv), Mail(q_send, q_recv), Mail(o_send, o_recv), Mail(x_send, x_recv)
    base_s, base_c = heads, 2 * heads

    def lines(index):
        return pl.ds(pl.multiple_of(index * rows, rows), rows)

    def kv_at(index, j=0):
        return W.at[j, lines(index), 0:KV]

    def q_at(index, j=0):
        return W.at[j, lines(index), KV:]

    def o_at(index, j=0):
        if len(WO.shape) == 4:
            return WO.at[j, index]
        return WO.at[j, :, pl.ds(pl.multiple_of(index * cols, cols), cols)]

    def kv_from(m, j=0):
        place = lines(me)
        return [
            (wk.at[:, pl.ds(pl.multiple_of(m * DK, DK), DK)], W.at[j, place, 0:DK]),
            (wv.at[:, pl.ds(pl.multiple_of(m * DV, DV), DV)], W.at[j, place, DK:KV]),
        ]

    def q_from(m, j=0):
        return [(wq.at[:, pl.ds(pl.multiple_of(m * DK, DK), DK)], W.at[j, lines(me), KV:])]

    def o_from(m, j=0):
        return [(wo.at[pl.ds(pl.multiple_of(m * DV, DV), DV), :], o_at(me, j))]

    plane = me // 4
    y_peer = (plan.flip(me, 2), core)

    def tag(dz, q, kind):
        return ((dz + 3) * 2 + q) * 3 + kind

    def source(dz, q, y):
        return plan.flip(me, q + 2 * y) + 4 * dz

    def room(sign):
        return (3 - plane, plane) if sign > 0 else (plane, 3 - plane)

    def line_open(box, pairs):
        for j in (0, 1):
            for src, dst in pairs(plan.other(mine, 1 + 2 * j), j):
                box.send(src, dst, (peers[1], core), tag(0, 1, j))

    def line_own_y(box, pairs):
        for src, dst in pairs(mine, 0):
            box.send(src, dst, y_peer, tag(0, 0, 2))

    def line_own_z(box, pairs):
        for j in (1, 0):
            for sign in (1, -1):
                test = room(sign)[0] >= 2 - j
                copies = [
                    box.send(src, dst, (me + 4 * sign, core), tag(-sign, 0, 1 - j), True, test)
                    for src, dst in pairs(plan.other(mine, 2 * j), 1 - j)
                ]
                start_if(test, copies)

    def line_x_y(box, view):
        for j in (0, 1):
            index = source(0, 1, 0)
            box.receive(view(index, j), (peers[1], core), tag(0, 1, j))
            if j == 0:
                box.send(view(index), view(index), y_peer, tag(0, 1, 2))

    def line_x_z(box, view):
        index = source(0, 1, 0)
        for j in (0, 1):
            for sign in (1, -1):
                test = room(sign)[0] >= 2 - j
                start_if(test, [
                    box.send(view(index, j), view(index, 1 - j), (me + 4 * sign, core), tag(-sign, 1, 1 - j), True, test)
                ])

    def line_step(box, view, k, q):
        for sign in (1, -1):
            ahead, behind = room(sign)
            for j in (0, 1):
                if k + j > 3:
                    continue
                index = source(-sign * k, q, 0)
                test = (behind >= k) & (ahead >= j)
                onward = (behind >= k) & (ahead >= 2 - j)
                over = [box.send(view(index), view(index), y_peer, tag(-sign * k, q, 2), True, test)] if j == 0 else []
                on = []
                if k + 2 - j <= 3:
                    on.append(
                        box.send(
                            view(index, j), view(index, 1 - j), (me + 4 * sign, core),
                            tag(-sign * (k + 1), q, 1 - j), True, onward,
                        )
                    )

                @pl.when(test)
                def _():
                    box.receive(view(index, j), (me - 4 * sign, core), tag(-sign * k, q, j))
                    for copy in over:
                        copy.start()

                if on:
                    start_if(onward, on)

    def line_await(box, view, gaps):
        for dz in gaps:
            for q in (0, 1):
                test = (plane + dz >= 0) & (plane + dz <= 3)

                @pl.when(test)
                def _():
                    box.receive(view(source(dz, q, 1)), y_peer, tag(dz, q, 2))

    def to_team(box, pairs):
        for d in range(1, heads):
            for src, dst in pairs(plan.member(peers[d])):
                box.send(src, dst, (peers[d], core), plan.mask(d))

    def own_out(box, pairs, bits, held=False):
        return [
            box.send(src, dst, (plan.flip(me, b), core), b, held) for b in bits for src, dst in pairs(mine)
        ]

    def start_if(test, copies):
        @pl.when(test)
        def _():
            for copy in copies:
                copy.start()

    def await_piece(box, view, s, d):
        if s == 0 and d == 0:
            return
        mask = s | plan.mask(d)
        hop = plan.hop(s)
        sender = peers[d] if hop < 0 else plan.flip(me, plan.span[hop])
        box.receive(view(plan.flip(me, mask)), (sender, core), mask)

    def hand_over(box, view, s, d):
        mask = s | plan.mask(d)
        source = plan.flip(me, mask)
        for later in range(plan.hop(s) + 1, last_hop + 1):
            bit = plan.span[later]
            box.send(view(source), view(source), (plan.flip(me, bit), core), mask ^ bit)

    def forward(box, view, s, d):
        await_piece(box, view, s, d)
        hand_over(box, view, s, d)

    def slot_rows(member, c):
        return pl.ds(pl.multiple_of((member * tp + c) * share, share), share)

    def slot(index, c):
        return X.at[slot_rows(plan.member(index), c), :]

    locals_ = []
    for at, (src, dst) in enumerate(kv_from(mine) + q_from(mine) + o_from(mine)):
        copy = pltpu.make_async_copy(src, dst, local_sem.at[at])
        copy.start()
        locals_.append(copy)
    line = plan.line
    if line:
        line_open(mail_kv, kv_from)
        line_own_y(mail_kv, kv_from)
        line_own_z(mail_kv, kv_from)
        line_open(mail_q, q_from)
        line_own_y(mail_q, q_from)
    else:
        to_team(mail_kv, kv_from)
        own_out(mail_kv, kv_from, plan.span)
        to_team(mail_q, q_from)
        own_out(mail_q, q_from, plan.span)
    raw = tokens[...].astype(jnp.float32)
    raw = raw * lax.rsqrt(jnp.mean(raw * raw, axis=-1, keepdims=True) + EPS) * gain[...]
    X[slot_rows(mine, core), :] = raw.astype(jnp.bfloat16)
    SH[mine] = jnp.broadcast_to(shift[...], SH.shape[1:])

    def token_on(d, top):
        for k in range(top):
            mail_x.send(slot(peers[d], core), slot(peers[d], core), (peers[1 << k], core), d ^ (1 << k))
        for e, c in enumerate(cores):
            mail_x.send(slot(peers[d], core), slot(peers[d], core), (me, c), base_c + d * (tp - 1) + e)

    def token_in(d):
        k = d.bit_length() - 1
        low = (d & -d).bit_length() - 1
        mail_x.receive(slot(peers[d], core), (peers[1 << low], core), d)
        token_on(d, low)

    def token_ready(d):
        for e, c in enumerate(back):
            mail_x.receive(slot(peers[d], c), (me, c), base_c + d * (tp - 1) + e)
        if d:
            mail_x.receive(SH.at[plan.member(peers[d])], (peers[d], core), base_s + d)

    token_on(0, len(plan.team))
    for d in range(1, heads):
        mail_x.send(SH.at[mine], SH.at[mine], (peers[d], core), base_s + d)
    for copy in locals_:
        copy.wait()

    tile = min(seg, 256)
    tiles = seg // tile
    row = lax.broadcasted_iota(jnp.int32, (tile, tile), 0)
    col = lax.broadcasted_iota(jnp.int32, (tile, tile), 1)
    lower = (row >= col) & (row // BLOCK == col // BLOCK)
    ones = jnp.where(lower, 1.0, 0.0).astype(jnp.bfloat16)
    causal = lax.broadcasted_iota(jnp.int32, (BLOCK, BLOCK), 0) >= lax.broadcasted_iota(jnp.int32, (BLOCK, BLOCK), 1)
    up_here = up[:, pl.ds(pl.multiple_of(mine * DK, DK), DK)]
    bias_here = bias[:, pl.ds(pl.multiple_of(mine * DK, DK), DK)]

    def gates(d, t):
        i = plan.other(mine, d)
        at = pl.ds(pl.multiple_of(i * seg + t * tile, tile), tile)
        rank = lax.dot_general(X[at, :], down[...], NT, preferred_element_type=jnp.float32)
        pre = jnp.dot(rank.astype(jnp.bfloat16), up_here, preferred_element_type=jnp.float32) + bias_here
        gate = (jnp.minimum(pre, 0.0) - jnp.log1p(jnp.exp(-jnp.abs(pre)))) / TAU
        moved = SH[i, 0:1, pl.ds(pl.multiple_of(t * tile, tile), tile)]
        first = gate.astype(jnp.bfloat16)
        rest = gate - first.astype(jnp.float32)
        second = rest.astype(jnp.bfloat16)
        third = (rest - second.astype(jnp.float32)).astype(jnp.bfloat16)
        G[at, :] = (
            jnp.dot(ones, first, preferred_element_type=jnp.float32)
            + jnp.dot(ones, second, preferred_element_type=jnp.float32)
            + jnp.dot(ones, third, preferred_element_type=jnp.float32)
            + jnp.sum(jnp.where(lower, moved, 0.0), axis=1, keepdims=True)
        )

    def gates_of(low, high):
        def body(step, nothing):
            gates(low + step // tiles, step % tiles)
            return nothing

        lax.fori_loop(0, (high - low) * tiles, body, 0)

    def term(at, s, lo, hi):
        if staged:
            value = None
            for t in range(heads // run):
                place = plan.base(plan.flip(me, s), t) * rows
                span = pl.ds(pl.multiple_of(place, rows * run), rows * run)
                one = jnp.dot(X[at, span], W[0, span, lo:hi], preferred_element_type=jnp.float32)
                value = one if value is None else value + one
            return value
        return jnp.dot(X[at, :], W[0, :, lo:hi], preferred_element_type=jnp.float32)

    def accumulate(acc, lo, hi, s, first, low, high):
        def body(step, nothing):
            i = plan.other(mine, low + step // tiles)
            at = pl.ds(pl.multiple_of(i * seg + (step % tiles) * tile, tile), tile)
            value = term(at, s, lo, hi)
            acc[at, :] = value if first else acc[at, :] + value
            return nothing

        lax.fori_loop(0, (high - low) * tiles, body, 0)

    spread = plan.spread
    early = [s for s in spread if not s or plan.hop(s) < last_hop]
    late = [s for s in spread if s not in early]
    solo = [1 << k for k in range(len(plan.team))]
    rest = [d for d in range(1, heads) if d not in solo]
    waiting = [(s, d) for s in early if s for d in range(heads)]
    if line:
        line_x_y(mail_kv, kv_at)
        line_x_z(mail_kv, kv_at)
        line_step(mail_kv, kv_at, 1, 0)
        token_ready(0)
        gates_of(0, 1)
        line_x_y(mail_q, q_at)
        line_own_y(mail_o, o_from)
        for d in solo:
            token_in(d)
        line_step(mail_kv, kv_at, 1, 1)
        line_open(mail_o, o_from)
        token_ready(1)
        gates_of(1, 2)
        line_step(mail_kv, kv_at, 2, 0)
        token_ready(2)
        gates_of(2, 3)
        line_step(mail_kv, kv_at, 2, 1)
        line_own_z(mail_q, q_from)
        line_x_z(mail_q, q_at)
        token_in(3)
        accumulate(acc_kv, 0, KV, spread[0], True, 0, 3)
        line_step(mail_kv, kv_at, 3, 0)
        token_ready(3)
        gates_of(3, 4)
        accumulate(acc_kv, 0, KV, spread[0], True, 3, 4)
        line_step(mail_kv, kv_at, 3, 1)
        line_step(mail_q, q_at, 1, 0)
        line_step(mail_q, q_at, 1, 1)
        accumulate(acc_kv, 0, KV, spread[1], False, 0, heads)
        line_await(mail_kv, kv_at, (0, 1, -1))
        line_step(mail_q, q_at, 2, 0)
        line_step(mail_q, q_at, 2, 1)
        line_own_z(mail_o, o_from)
        line_x_y(mail_o, o_at)
        line_x_z(mail_o, o_at)
        accumulate(acc_kv, 0, KV, spread[2], False, 0, heads)
        line_step(mail_q, q_at, 3, 0)
        line_step(mail_q, q_at, 3, 1)
        line_await(mail_kv, kv_at, (2, -2, 3, -3))
    else:
        for d in range(1, heads):
            forward(mail_kv, kv_at, 0, d)
        token_ready(0)
        gates_of(0, 1)
        for d in range(1, heads):
            forward(mail_q, q_at, 0, d)
        to_team(mail_o, o_from)
        for d in solo:
            token_in(d)
        for d in solo:
            token_ready(d)
            gates_of(d, d + 1)
        for s, e in waiting:
            forward(mail_kv, kv_at, s, e)
    if not line:
        near_heads = 3 if heads > 2 else heads
        for d in rest:
            token_in(d)
        if staged:
            for at, s in enumerate(spread[:-1]):
                if s in late:
                    for d in range(heads):
                        await_piece(mail_kv, kv_at, s, d)
                accumulate(acc_kv, 0, KV, s, at == 0, 0, near_heads)
        for d in rest:
            token_ready(d)
            gates_of(d, d + 1)
        for s, e in waiting:
            forward(mail_q, q_at, s, e)
        if staged:
            for at, s in enumerate(spread[:-1]):
                accumulate(acc_kv, 0, KV, s, at == 0, near_heads, heads)
            for d in range(heads):
                await_piece(mail_kv, kv_at, spread[-1], d)
        else:
            for s in late:
                for d in range(heads):
                    await_piece(mail_kv, kv_at, s, d)

    per_run = run * tiles
    ends[...] = jnp.zeros_like(ends)
    logs[...] = jnp.zeros_like(logs)

    def keys(index, nothing):
        u = index // per_run
        at = pl.ds(pl.multiple_of(index * tile, tile), tile)
        joined = term(at, spread[-1], 0, KV)
        if staged:
            joined = joined + acc_kv[at, :]
        joined = joined.astype(jnp.bfloat16)
        Kb[at, :] = joined[:, :DK]
        Vb[at, :] = joined[:, DK:]
        carry, past = ends[u], logs[u, 0:1, :]
        for b in range(tile // BLOCK):
            here = slice(b * BLOCK, (b + 1) * BLOCK)
            place = pl.ds(pl.multiple_of(index * tile + b * BLOCK, BLOCK), BLOCK)
            cumul = G[place, :]
            final = cumul[BLOCK - 1 : BLOCK]
            carries[index * (tile // BLOCK) + b] = carry.astype(jnp.bfloat16)
            decayed = (joined[here, :DK].astype(jnp.float32) * jnp.exp(final - cumul)).astype(jnp.bfloat16)
            carry = jnp.exp(final) * carry + lax.dot_general(
                joined[here, DK:], decayed, TN, preferred_element_type=jnp.float32
            )
            past = past + final
        ends[u] = carry
        logs[u] = jnp.broadcast_to(past, logs.shape[1:])
        return nothing

    lax.fori_loop(0, heads * tiles, keys, 0)

    mail_s = Mail(s_send, s_recv)
    depth = DV // CHUNKS

    def scan(c):
        piece = slice(c * depth, (c + 1) * depth)
        ahead = [jnp.zeros((1, DK), jnp.float32)] * blocks
        spans = [logs[u, 0:1, :] for u in range(blocks)]
        groups = [[u] for u in range(blocks)]
        for u in range(blocks):
            hold[u, piece, :] = jnp.zeros((depth, DK), jnp.float32)
        at = 0
        for bit in plan.bits:
            if bit < run:
                continue
            if bit in plan.team:
                merged, span = [], []
                for a in range(0, len(groups), 2):
                    one, two = groups[a], groups[a + 1]
                    value = ends[one[0], piece, :]
                    for i in two:
                        hold[i, piece, :] = hold[i, piece, :] + jnp.exp(ahead[i]) * value
                        ahead[i] = ahead[i] + spans[a]
                    ends[one[0], piece, :] = jnp.exp(spans[a + 1]) * value + ends[two[0], piece, :]
                    span.append(spans[a] + spans[a + 1])
                    merged.append(one + two)
                groups, spans = merged, span
                continue
            partner = (plan.flip(me, bit), core)
            high = (me // bit) % 2 == 1
            final = bit == plan.bits[-1]
            low = jnp.logical_not(high) if final else None
            for u, g in enumerate(groups):
                if c == 0:
                    sent_log[at + u] = jnp.broadcast_to(spans[u], sent_log.shape[1:])
                    mail_s.send(
                        sent_log.at[at + u], got_log.at[at + u], partner, (CHUNKS + 1) * (at + u), final, low
                    )
                    if final:
                        start_if(low, [mail_s.out[-1][0]])
                sent[at + u, piece, :] = ends[g[0], piece, :].astype(jnp.bfloat16)
                mail_s.send(
                    sent.at[at + u, piece, :], got.at[at + u, piece, :], partner, (CHUNKS + 1) * (at + u) + 1 + c,
                    final, low,
                )
                if final:
                    start_if(low, [mail_s.out[-1][0]])
            yield
            if final:

                @pl.when(high)
                def _():
                    for u, g in enumerate(groups):
                        if c == 0:
                            mail_s.receive(got_log.at[at + u], partner, (CHUNKS + 1) * (at + u))
                        mail_s.receive(got.at[at + u, piece, :], partner, (CHUNKS + 1) * (at + u) + 1 + c)
                        value = got[at + u, piece, :].astype(jnp.float32)
                        for i in g:
                            hold[i, piece, :] = hold[i, piece, :] + jnp.exp(ahead[i]) * value

                continue
            for u, g in enumerate(groups):
                if c == 0:
                    mail_s.receive(got_log.at[at + u], partner, (CHUNKS + 1) * (at + u))
                mail_s.receive(got.at[at + u, piece, :], partner, (CHUNKS + 1) * (at + u) + 1 + c)
                value = got[at + u, piece, :].astype(jnp.float32)
                value_log = got_log[at + u, 0:1, :]
                for i in g:
                    hold[i, piece, :] = hold[i, piece, :] + jnp.where(high, jnp.exp(ahead[i]), 0.0) * value
                    ahead[i] = ahead[i] + jnp.where(high, value_log, 0.0)
                ends[g[0], piece, :] = (
                    jnp.exp(jnp.where(high, 0.0, value_log)) * ends[g[0], piece, :]
                    + jnp.exp(jnp.where(high, spans[u], 0.0)) * value
                )
                spans[u] = spans[u] + value_log
            at += len(groups)
        for u in range(blocks):
            starts[u, piece, :] = hold[u, piece, :].astype(jnp.bfloat16)
        yield

    scans = [scan(c) for c in range(CHUNKS)]
    steps = len([b for b in plan.bits if b not in plan.team])

    def step_scans():
        for one in scans:
            next(one)

    step_scans()
    cut = (heads + 1) // 2
    if line:
        line_step(mail_o, o_at, 1, 0)
    else:
        own_out(mail_o, o_from, plan.span[::-1])
        for d in range(1, cut):
            forward(mail_o, o_at, 0, d)
        for s in late:
            for d in range(heads):
                await_piece(mail_q, q_at, s, d)

    def queries(index, nothing):
        u = index // per_run
        at = pl.ds(pl.multiple_of(index * tile, tile), tile)
        joined = term(at, spread[0], KV, KV + DK)
        if staged:
            for s in spread[1:]:
                joined = joined + term(at, s, KV, KV + DK)
        joined = joined.astype(jnp.bfloat16).astype(jnp.float32) * DK ** (-0.5)
        past = acc_q[0:1, :]
        past = jnp.where(index % per_run == 0, 0.0, past)
        for b in range(tile // BLOCK):
            here = slice(b * BLOCK, (b + 1) * BLOCK)
            place = pl.ds(pl.multiple_of(index * tile + b * BLOCK, BLOCK), BLOCK)
            q = joined[here]
            k = Kb[place, :].astype(jnp.float32)
            cumul = G[place, :]
            centre = cumul - cumul[BLOCK // 2 : BLOCK // 2 + 1]
            final = cumul[BLOCK - 1 : BLOCK]
            q_scaled = (q * jnp.exp(centre)).astype(jnp.bfloat16)
            k_scaled = (k * jnp.exp(-centre)).astype(jnp.bfloat16)
            scores = lax.dot_general(q_scaled, k_scaled, NT, preferred_element_type=jnp.float32)
            scores = jnp.where(causal, scores, 0.0).astype(jnp.bfloat16)
            near = (q * jnp.exp(cumul)).astype(jnp.bfloat16)
            within[place, :] = jnp.dot(scores, Vb[place, :], preferred_element_type=jnp.float32) + lax.dot_general(
                near, carries[index * (tile // BLOCK) + b], NT, preferred_element_type=jnp.float32
            )
            reach[place, :] = (q * jnp.exp(cumul + past)).astype(jnp.bfloat16)
            past = past + final
        acc_q[0:1, :] = past
        return nothing

    acc_q[...] = jnp.zeros_like(acc_q)
    middle = heads * tiles // 2
    if line:
        for c, one in enumerate(scans):
            next(one)
    else:
        lax.fori_loop(0, middle, queries, 0)
        if steps:
            step_scans()
    if line:
        line_step(mail_o, o_at, 1, 1)
        line_await(mail_q, q_at, (0, 1, -1, 2, -2, 3, -3))
    else:
        for d in range(max(cut, 1), heads):
            forward(mail_o, o_at, 0, d)
    lax.fori_loop(0 if line else middle, heads * tiles, queries, 0)
    if line:
        line_step(mail_o, o_at, 2, 0)
        line_step(mail_o, o_at, 2, 1)
    else:
        for s in early:
            if s:
                for d in range(cut):
                    forward(mail_o, o_at, s, d)
    for _ in range(steps - 1):
        step_scans()

    def shape(index, nothing):
        u = index // per_run
        at = pl.ds(pl.multiple_of(index * tile, tile), tile)
        wide = within[at, :] + lax.dot_general(reach[at, :], starts[u], NT, preferred_element_type=jnp.float32)
        value = wide * lax.rsqrt(jnp.mean(wide * wide, axis=-1, keepdims=True) + EPS) * out_gain[...]
        value = value.astype(jnp.bfloat16)
        if tile == seg:
            for c in range(tp):
                to = pl.ds(pl.multiple_of((c * heads + index) * share, share), share)
                shaped[to, :] = value[c * share : (c + 1) * share]
        else:
            for p in range(tile // share):
                lot = index * (tile // share) + p
                to = pl.ds(pl.multiple_of(((lot % tp) * heads + lot // tp) * share, share), share)
                shaped[to, :] = value[p * share : (p + 1) * share]
        return nothing

    lax.fori_loop(0, heads * tiles, shape, 0)

    mail_r = Mail(r_send, r_recv)
    lots = heads * share
    width = out.shape[1]
    groups = [[s] for s in spread] if staged else [spread]
    fields = heads // run

    def product(c, group):
        left = shaped[pl.ds(pl.multiple_of(c * lots, lots), lots), :]
        if staged:
            right = []
            for t in range(fields):
                place = plan.base(plan.flip(me, group[0]), t) * cols
                right.append(WO[0, :, pl.ds(pl.multiple_of(place, run * cols), run * cols)])
            return [jnp.dot(left, one, preferred_element_type=jnp.float32) for one in right]
        if len(WO.shape) == 4:
            return [jnp.dot(left, WO[0, s], preferred_element_type=jnp.float32) for s in range(n)]
        return [jnp.dot(left, WO[0], preferred_element_type=jnp.float32)]

    def spots(values):
        at, result = 0, []
        for value in values:
            result.append(slice(at, at + value.shape[1]))
            at += value.shape[1]
        return result

    per_group = heads * tp + heads

    def lot_of(d):
        return pl.ds(pl.multiple_of(plan.member(peers[d]) * share, share), share)

    def for_others(g):
        for e, c in enumerate(cores):
            values = product(c, groups[g])
            for place, value in zip(spots(values), values):
                part[g, e, :, place] = value.astype(jnp.bfloat16)
            mail_r.send(part.at[g, e], from_core.at[g, e], (me, c), g * per_group + e)

    def for_self(g):
        values = product(core, groups[g])
        for place, value in zip(spots(values), values):
            total[g, :, place] = value

    def add_cores(g):
        for e, c in enumerate(back):
            mail_r.receive(from_core.at[g, e], (me, c), g * per_group + e)
            total[g] = total[g] + from_core[g, e].astype(jnp.float32)
        if heads > 1:
            sum_out[g] = total[g].astype(jnp.bfloat16)

    def place_out(g, value):
        if staged:
            for t in range(fields):
                place = plan.base(plan.flip(me, groups[g][0]), t) * cols
                out[:, pl.ds(pl.multiple_of(place, run * cols), run * cols)] = value[:, t * run * cols : (t + 1) * run * cols]
        else:
            out[...] = value

    if line:
        half = out.shape[1] // len(groups) // 2
        sides = [slice(0, half), slice(half, 2 * half)]

        def pass_far(g):
            for d in (1, 2):
                mail_r.send(
                    sum_out.at[g, lot_of(3), sides[d - 1]], relay.at[g, d - 1], (peers[d], core), g * per_group + tp + d
                )

        def send_near(g):
            for d in (1, 2):
                mail_r.receive(relay.at[g, d - 1], (peers[d], core), g * per_group + tp + d)
                to = lot_of(3 - d)
                sum_out[g, to, sides[d - 1]] = (
                    total[g, to, sides[d - 1]] + relay[g, d - 1].astype(jnp.float32)
                ).astype(jnp.bfloat16)
                mail_r.send(
                    sum_out.at[g, to, :], sum_in.at[g, 2 - d], (peers[3 - d], core), g * per_group + tp + 5 - d
                )

        for_others(0)
        for_self(0)
        line_step(mail_o, o_at, 3, 0)
        line_step(mail_o, o_at, 3, 1)
        for_others(1)
        add_cores(0)
        pass_far(0)
        for_self(1)
        add_cores(1)
        pass_far(1)
        send_near(0)
        line_await(mail_o, o_at, (0, 1, -1))
        for_others(2)
        send_near(1)
        for_self(2)
        add_cores(2)
        pass_far(2)
        line_await(mail_o, o_at, (2, -2, 3, -3))
        for_others(3)
        send_near(2)
        for_self(3)
        add_cores(3)
        pass_far(3)
        send_near(3)
        for g in range(len(groups)):
            value = total[g, lot_of(0), :]
            for d in (1, 2):
                mail_r.receive(sum_in.at[g, d - 1], (peers[d], core), g * per_group + tp + 2 + d)
                value = value + sum_in[g, d - 1].astype(jnp.float32)
            place_out(g, value.astype(jnp.bfloat16))
    else:
        for g, group in enumerate(groups):
            for s in group:
                if s in late:
                    for d in range(heads):
                        await_piece(mail_o, o_at, s, d)
                elif s:
                    for d in range(cut, heads):
                        forward(mail_o, o_at, s, d)
            for_others(g)
            for_self(g)
            add_cores(g)
            for d in range(heads - 1, 0, -1):
                mail_r.send(
                    sum_out.at[g, lot_of(d), :], sum_in.at[g, d - 1], (peers[d], core), g * per_group + heads * tp + d
                )
        for g in range(len(groups)):
            value = total[g, lot_of(0), :]
            for d in range(heads - 1, 0, -1):
                mail_r.receive(sum_in.at[g, d - 1], (peers[d], core), g * per_group + heads * tp + d)
                value = value + sum_in[g, d - 1].astype(jnp.float32)
            place_out(g, value.astype(jnp.bfloat16))
    for box in (mail_kv, mail_q, mail_o, mail_x, mail_s, mail_r):
        box.finish()


def on_device(
    tokens, norm_gain, w_query, w_key, w_value, w_rank_down, w_rank_up, gate_bias, decay_shift, out_gain, w_out
):
    n, tp = lax.axis_size("sp"), lax.axis_size("tp")
    heads = w_query.shape[1] // DK
    plan = Plan(n, tp, heads)
    rows, width = tokens.shape
    deep = w_query.shape[0]
    seg = rows * tp
    count = heads * seg
    dma, vmem = pltpu.SemaphoreType.DMA, pltpu.VMEM
    cols = w_out.shape[1]
    aligned = cols % 128 == 0
    staged = aligned and len(plan.span) > 0 and plan.run * deep % 256 == 0
    groups = len(plan.spread) if staged else 1
    field = width // groups
    sides = 2 if plan.line else 1
    posts = 42 if plan.line else n
    most = max(1, plan.blocks * len(plan.span))
    given = max(1, tp - 1)
    bf16, f32 = jnp.bfloat16, jnp.float32
    slots = 80 if plan.line else 2 * n + 8 * (heads + len(plan.span))
    tokens_sent = heads * (tp + 2 + len(plan.team))
    return pl.pallas_call(
        functools.partial(layer_kernel, plan, staged),
        out_shape=jax.ShapeDtypeStruct((rows, width), bf16),
        in_specs=[VMEM] * 11,
        out_specs=VMEM,
        scratch_shapes=[
            vmem((count, width), bf16),
            vmem((heads, 8, seg), f32),
            vmem((sides, n * deep, KV + DK), bf16),
            vmem((sides, DV, n * cols) if aligned else (sides, n, DV, cols), bf16),
            vmem((count, KV) if staged else (8, 128), f32),
            vmem((8, DK), f32),
            vmem((count, DK), f32),
            vmem((count, DK), bf16),
            vmem((count, DV), bf16),
            vmem((count // BLOCK, DV, DK), bf16),
            vmem((count, DV), f32),
            vmem((count, DK), bf16),
            vmem((plan.blocks, DV, DK), f32),
            vmem((plan.blocks, 8, DK), f32),
            vmem((plan.blocks, DV, DK), f32),
            vmem((plan.blocks, DV, DK), bf16),
            vmem((most, DV, DK), bf16),
            vmem((most, DV, DK), bf16),
            vmem((most, 8, DK), f32),
            vmem((most, 8, DK), f32),
            vmem((count, DV), bf16),
            vmem((groups, given, heads * rows, field), bf16),
            vmem((groups, given, heads * rows, field), bf16),
            vmem((groups, heads * rows, field), f32),
            vmem((groups, heads * rows, field) if heads > 1 else (1, 16, 128), bf16),
            vmem((groups, max(1, heads - 1), rows, field) if heads > 1 else (1, 1, 16, 128), bf16),
            vmem((groups, 2, rows, field // 2) if plan.line else (1, 1, 16, 128), bf16),
            dma((slots,)),
            dma((posts,)),
            dma((slots,)),
            dma((posts,)),
            dma((slots,)),
            dma((posts,)),
            dma((tokens_sent,)),
            dma((heads * (tp + 2),)),
            dma(((CHUNKS + 1) * most,)),
            dma(((CHUNKS + 1) * most,)),
            dma((groups * (heads + tp),)),
            dma((groups * (heads * tp + heads),)),
            dma((4,)),
        ],
        compiler_params=pltpu.CompilerParams(
            collective_id=0, has_side_effects=True, vmem_limit_bytes=LIMIT
        ),
        name="layer",
    )(
        tokens,
        norm_gain[None],
        decay_shift[None],
        w_query,
        w_key,
        w_value,
        w_out,
        w_rank_down.T,
        w_rank_up,
        gate_bias[None],
        out_gain[None],
    )


def solution(mesh):
    return jax.shard_map(
        on_device,
        mesh=mesh,
        in_specs=(
            P(("sp", "tp"), None),
            P(),
            P("sp", "tp"),
            P("sp", "tp"),
            P("sp", "tp"),
            P(),
            P(None, "tp"),
            P("tp"),
            P("sp"),
            P(),
            P("tp", "sp"),
        ),
        out_specs=P(("sp", "tp"), None),
        check_vma=False,
    )
```
